512 devices in a mesh: sp: 16 (over z), fs: 4 (over y), tp: 8 (over x, core).
Axes of the slice: x: 4, y: 4, z: 16, core: 2. Of those that a mesh axis runs over, the one named last changes fastest.
Arguments:
- inputs: bfloat16 [4, 2048, 2048], P('fs', 'sp'), may hold values from -9 to 9
- norm_gain: float32 [2048], replicated, may hold values from 0.1 to 1.9
- hg_query_w: bfloat16 [2048, 1024], P(('sp', 'fs'), 'tp'), may hold values from -0.125 to 0.125
- hg_fwd_w: bfloat16 [2048, 1024], P(('sp', 'fs'), 'tp'), may hold values from -0.125 to 0.125
- hg_bwd_w: bfloat16 [2048, 1024], P(('sp', 'fs'), 'tp'), may hold values from -0.125 to 0.125
- hg_value_w: bfloat16 [2048, 1024], P(('sp', 'fs'), 'tp'), may hold values from -0.125 to 0.125
- floor_gap: float32 [2, 1024], P(None, 'tp'), may hold values from 0 to 0.1
- hg_norm_gain: float32 [64], replicated, may hold values from 0.1 to 1.9
- df_query_w: bfloat16 [2048, 512], P(('sp', 'fs'), 'tp'), may hold values from -0.176776695 to 0.176776695
- df_key_w: bfloat16 [2048, 512], P(('sp', 'fs'), 'tp'), may hold values from -4.4194174 to 4.4194174
- df_value_w: bfloat16 [2048, 512], P(('sp', 'fs'), 'tp'), may hold values from -0.125 to 0.125
- diff_lambda: float32 [8], P('tp'), may hold values from 0.3 to 0.8
- df_norm_gain: float32 [64], replicated, may hold values from 0.1 to 1.9
- out_hg_w: bfloat16 [1024, 2048], P('tp'), may hold values from -0.15625 to 0.15625
- out_df_w: bfloat16 [512, 2048], P('tp'), may hold values from -0.15625 to 0.15625
- post_gain: float32 [2048], replicated, may hold values from 0.1 to 1.9
Outputs:
- mixed: bfloat16 [4, 2048, 2048], P('fs', ('sp', 'tp'))
The draws below stay inside these ranges and needn't reach their ends.
All inputs are finite; a program needn't handle non-finite values.
Results may differ from the reference program's by a relative error of at most 0.017.
Values may be sent and summed in bfloat16 or wider, within the bound.
No kernel may reach another device: no remote copies, remote signals or barrier semaphores. Data moves between devices by JAX's collectives and lax.ppermute only.
A program may use at most 64 MiB of HBM per device.

```python
import math
import jax
import jax.numpy as jnp
from jax import lax

D = 2048
HG_HEADS = 16
HEAD = 64
DF_HEADS = 8
DQK = 32
BLOCK = 64
TOK_DEV = 128
DFV = 64
HG_WIDTH = 1024
DF_QK_WIDTH = 512
DF_WIDTH = 512
SEQ = 2048
BATCH = 4
N_TP = 8


def draw_inputs(key, part):
    base_key, shift_key = jax.random.split(key)
    base_draw = jax.random.normal(base_key, (BATCH, SEQ, D), jnp.float32)
    shifts = jax.random.normal(shift_key, (BATCH, SEQ // TOK_DEV, D), jnp.float32)
    summed = base_draw + jnp.repeat(shifts, TOK_DEV, axis=1)
    return jnp.clip(summed, -9.0, 9.0).astype(jnp.bfloat16)


def draw_floor_gap(key, part):
    kind_key, slow_key, fast_key = jax.random.split(key, 3)
    chooser = jax.random.randint(kind_key, (2, HG_HEADS, 1), 0, 10)
    is_fast = chooser < 5
    slow_gap = jnp.exp(jax.random.uniform(slow_key, (2, HG_HEADS, HEAD), jnp.float32, math.log(0.1), 0.0)) / SEQ
    fast_gap = jnp.exp(jax.random.uniform(fast_key, (2, HG_HEADS, HEAD), jnp.float32, math.log(0.03), math.log(0.1)))
    return jnp.where(is_fast, fast_gap, slow_gap).reshape(2, HG_HEADS * HEAD).astype(jnp.float32)


def query_key_pair(key):
    base_key = jax.random.fold_in(key, 17)
    first_key, second_key = jax.random.split(base_key)
    scale_w = 1.3 * D ** (-0.5)
    queries_w = jnp.clip(jax.random.normal(first_key, (D, DF_QK_WIDTH), jnp.float32), -6.0, 6.0) * scale_w
    noise_w = jnp.clip(jax.random.normal(second_key, (D, DF_QK_WIDTH), jnp.float32), -6.0, 6.0) * scale_w
    keys_w = noise_w
    return (queries_w, keys_w)


def draw_df_query_w(key, part):
    return query_key_pair(key)[0].astype(jnp.bfloat16)


def draw_df_key_w(key, part):
    return query_key_pair(key)[1].astype(jnp.bfloat16)


def levels(key, extent, shards, smallest, high):
    level, own = 1.0, jax.random.fold_in(key, 6)
    for position, parts in shards:
        heights = jnp.exp(jax.random.uniform(jax.random.fold_in(own, position), (parts,), jnp.float32, smallest / len(shards), high / len(shards)))
        level = level * jnp.repeat(heights, extent[position] // parts).reshape([-1 if axis == position else 1 for axis in range(len(extent))])
    return level


def scatter_about(key, extent, width, limit, cuts=(), kind=jnp.bfloat16):
    values = jax.random.normal(key, extent, jnp.float32) * width
    if len(cuts) > 0:
        values = levels(key, extent, cuts, -0.22, 0.18) * values
    return jnp.clip(values, min=-limit, max=limit).astype(kind)


def setup_inputs(seed: int = 0) -> dict:
    arg_keys = jax.random.split(jax.random.key(seed), 17)
    return {
        "inputs": draw_inputs(jax.random.fold_in(arg_keys[16], 71), 0),
        "norm_gain": jnp.clip(1.0 + 0.18 * jax.random.normal(arg_keys[1], (D,), jnp.float32), 0.1, 1.9),
        "hg_query_w": scatter_about(arg_keys[2], (D, HG_WIDTH), D ** -0.5, 0.125, ((0, 64), (1, 8))),
        "hg_fwd_w": scatter_about(arg_keys[3], (D, HG_WIDTH), D ** -0.5, 0.125, ((0, 64), (1, 8))),
        "hg_bwd_w": scatter_about(arg_keys[4], (D, HG_WIDTH), D ** -0.5, 0.125, ((0, 64), (1, 8))),
        "hg_value_w": scatter_about(arg_keys[5], (D, HG_WIDTH), D ** -0.5, 0.125, ((0, 64), (1, 8))),
        "floor_gap": draw_floor_gap(jax.random.fold_in(arg_keys[16], 71), 0),
        "hg_norm_gain": jnp.clip(1.0 + 0.18 * jax.random.normal(arg_keys[7], (HEAD,), jnp.float32), 0.1, 1.9),
        "df_query_w": draw_df_query_w(jax.random.fold_in(arg_keys[16], 71), 0),
        "df_key_w": draw_df_key_w(jax.random.fold_in(arg_keys[16], 71), 0),
        "df_value_w": scatter_about(arg_keys[10], (D, DF_WIDTH), D ** -0.5, 0.125, ((0, 64), (1, 8))),
        "diff_lambda": jnp.clip(0.3 + 0.5 * jax.random.uniform(arg_keys[11], (DF_HEADS,), jnp.float32) ** levels(arg_keys[11], (DF_HEADS,), ((0, 8),), -0.2, 0.2), 0.3, 0.8),
        "df_norm_gain": jnp.clip(1.0 + 0.18 * jax.random.normal(arg_keys[12], (DFV,), jnp.float32), 0.1, 1.9),
        "out_hg_w": scatter_about(arg_keys[13], (HG_WIDTH, D), (HG_WIDTH + DF_WIDTH) ** -0.5, 0.15625, ((0, 8),)),
        "out_df_w": scatter_about(arg_keys[14], (DF_WIDTH, D), (HG_WIDTH + DF_WIDTH) ** -0.5, 0.15625, ((0, 8),)),
        "post_gain": jnp.clip(1.0 + 0.18 * jax.random.normal(arg_keys[15], (D,), jnp.float32), 0.1, 1.9),
    }


epsilon = 1e-06
df_factor = 0.8

def rms_scale(values):
    return lax.rsqrt(lax.optimization_barrier(jnp.mean(values * values, axis=-1, keepdims=True)) + epsilon)

def span_scan(queries, taken, values, kept_log):
    head_count, length, key_dim = queries.shape
    blocks = length // BLOCK

    def to_blocks(tensor):
        return tensor.reshape(head_count, blocks, BLOCK, tensor.shape[-1]).transpose(1, 0, 2, 3)
    lower_mask = jnp.tril(jnp.ones((BLOCK, BLOCK), dtype=bool))[:, :, None]
    highest_precision = lax.Precision.HIGHEST

    def advance(state_stack, pieces):
        query_block, key_block, value_block, g_blk = pieces
        cumulative_log = jnp.cumsum(g_blk, axis=1)
        across_blocks = jnp.einsum('bqy,byo->bqo', query_block * jnp.exp(cumulative_log), state_stack, precision=highest_precision)
        spread = cumulative_log[:, :, None, :] - cumulative_log[:, None, :, :]
        decays = jnp.where(lower_mask, jnp.exp(jnp.where(lower_mask, spread, 0.0)), 0.0)
        scores = jnp.einsum('hik,hijk->hij', query_block, decays * key_block[:, None, :, :], precision=highest_precision)
        inside = jnp.einsum('hij,hjv->hiv', scores, value_block, precision=highest_precision)
        final_log_decay = cumulative_log[:, -1:, :]
        carried = jnp.exp(final_log_decay[:, 0, :])[..., None] * state_stack
        fresh_portion = jnp.einsum('moc,moa->mca', key_block * jnp.exp(final_log_decay - cumulative_log), value_block, precision=highest_precision)
        return (carried + fresh_portion, across_blocks + inside)
    start_state = jnp.zeros((head_count, key_dim, values.shape[-1]), jnp.float32)
    final_state, outputs = lax.scan(advance, start_state, (to_blocks(queries), to_blocks(taken), to_blocks(values), to_blocks(kept_log)))
    return (outputs.transpose(1, 0, 2, 3).reshape(head_count, length, values.shape[-1]), final_state)

def reference(inputs, norm_gain, hg_query_w, hg_fwd_w, hg_bwd_w, hg_value_w, floor_gap, hg_norm_gain, df_query_w, df_key_w, df_value_w, diff_lambda, df_norm_gain, out_hg_w, out_df_w, post_gain):

    def one_sequence(tok_rows):
        rows_float = tok_rows.astype(jnp.float32)
        normed = (rows_float * rms_scale(rows_float) * norm_gain).astype(jnp.bfloat16)

        def project(weight):
            return jnp.dot(normed, weight, preferred_element_type=jnp.float32).astype(jnp.bfloat16)

        def split_heads(tensor):
            return tensor.astype(jnp.float32).reshape(SEQ, HG_HEADS, HEAD).transpose(1, 0, 2)
        queries = jax.nn.silu(split_heads(project(hg_query_w)))
        values = split_heads(project(hg_value_w))

        def direction(weight, gap_row, flipped):
            taken = gap_row.reshape(HG_HEADS, 1, HEAD) * jax.nn.sigmoid(-split_heads(project(weight)))
            series = (queries, taken, values, jnp.log1p(-taken))
            if flipped:
                series = tuple((jnp.flip(tensor, axis=1) for tensor in series))
            outputs, final_state = span_scan(*series)
            return jnp.flip(outputs, axis=1) if flipped else outputs
        recurrent = direction(hg_fwd_w, floor_gap[0], False) + direction(hg_bwd_w, floor_gap[1], True)
        hg_out = (recurrent * rms_scale(recurrent) * hg_norm_gain).transpose(1, 0, 2).reshape(SEQ, HG_WIDTH).astype(jnp.bfloat16)
        df_queries = project(df_query_w).reshape(SEQ // BLOCK, BLOCK, DF_HEADS, 2, DQK)
        df_keys = project(df_key_w).reshape(SEQ, DF_HEADS, 2, DQK).astype(jnp.float32)
        df_values = project(df_value_w).reshape(SEQ, DF_HEADS, DFV).astype(jnp.float32)

        def attend(query_block):
            scores = jnp.einsum('qhmd,khmd->hmqk', query_block.astype(jnp.float32), df_keys) * DQK ** (-0.5)
            shifted = jnp.exp(scores - lax.optimization_barrier(jnp.max(scores, axis=-1, keepdims=True)))
            totals = lax.optimization_barrier(jnp.sum(shifted, axis=-1))
            shifted_low = lax.optimization_barrier(shifted.astype(jnp.bfloat16)).astype(jnp.float32)
            accum = jnp.einsum('hmqk,khd->hmqd', shifted_low, df_values)
            return accum / totals[..., None]
        maps = lax.map(attend, df_queries)
        weighted = maps[:, :, 0] - diff_lambda[None, :, None, None] * maps[:, :, 1]
        df_out = (weighted * rms_scale(weighted) * df_norm_gain * df_factor).transpose(0, 2, 1, 3).reshape(SEQ, DF_WIDTH).astype(jnp.bfloat16)
        hg_parts = hg_out.reshape(SEQ, N_TP, HG_WIDTH // N_TP)
        df_parts = df_out.reshape(SEQ, N_TP, DF_WIDTH // N_TP)
        hg_rows = out_hg_w.reshape(N_TP, HG_WIDTH // N_TP, D)
        df_rows = out_df_w.reshape(N_TP, DF_WIDTH // N_TP, D)
        mixture = jnp.zeros((SEQ, D), jnp.float32)
        for member in range(N_TP):
            partial_sum = jnp.dot(hg_parts[:, member], hg_rows[member], preferred_element_type=jnp.float32) + jnp.dot(df_parts[:, member], df_rows[member], preferred_element_type=jnp.float32)
            mixture = mixture + lax.optimization_barrier(partial_sum.astype(jnp.bfloat16)).astype(jnp.float32)
        return (mixture * rms_scale(mixture) * post_gain).astype(jnp.bfloat16)
    return lax.map(one_sequence, inputs)
```

```python
import functools

import jax
import jax.numpy as jnp
from jax import lax
from jax.experimental import pallas as pl
from jax.experimental.pallas import tpu as pltpu
from jax.sharding import PartitionSpec as P

HEAD = 64
DQK = 32
LANES = 128
STATE_ROWS = 80

epsilon = 1e-06
df_factor = 0.8
f32 = jnp.float32
bf16 = jnp.bfloat16

SMEM_SPEC = pl.BlockSpec(memory_space=pltpu.SMEM)


def dot(a, b, dims, precision=None):
    return lax.dot_general(a, b, (dims, ((), ())), precision=precision, preferred_element_type=f32)


def pack_kernel(q, f, b, v, dq, dk, dv, out):
    copies, _, rows, _ = out.shape
    depth = q.shape[0]
    half = depth // 2
    for j, (wide, narrow) in enumerate(((q, dq), (f, dk), (b, dv), (v, dq))):
        folded = jnp.concatenate([narrow[:half, :], narrow[half:, :]], axis=1)
        block = jnp.concatenate([wide[...], folded], axis=0)
        for c in range(copies):
            out[c, j] = block


def norm_kernel(x, gain, out):
    rows = x[0].astype(f32)
    scale = lax.rsqrt(jnp.mean(rows * rows, axis=-1, keepdims=True) + epsilon)
    out[...] = (rows * scale * gain[...]).astype(bf16)


def project_kernel(places, own, before, after, far_top, far_low, weights, out, rhs):
    blocks, packed, _ = weights.shape
    depth = packed * 2 // 3
    half = depth // 2
    wide = weights[:, :depth, :]
    narrow = weights[:, depth:, :].astype(f32)
    first, second = narrow[:, :, :HEAD], narrow[:, :, HEAD:]
    narrow = jnp.concatenate(
        [
            jnp.concatenate([first, first], axis=2),
            jnp.concatenate([second, second], axis=2),
        ],
        axis=1,
    ).astype(bf16)
    rhs[:, :LANES] = wide.reshape(blocks * depth, LANES)
    rhs[:, LANES:] = narrow.reshape(blocks * depth, LANES)
    top = far_top.shape[0]
    for k, rows in enumerate((own, before, after)):
        out[places[k]] = dot(rows[...], rhs[...], ((1,), (0,))).astype(bf16)
    out[places[3], :top] = dot(far_top[...], rhs[...], ((1,), (0,))).astype(bf16)
    out[places[3], top:] = dot(far_low[...], rhs[...], ((1,), (0,))).astype(bf16)


def local_kernel(place, got, gaps, message, local, read_fwd, read_bwd):
    length = got.shape[1]
    devices = message.shape[0]
    me = place[0]
    row = lax.broadcasted_iota(jnp.int32, (length, length), 0)
    col = lax.broadcasted_iota(jnp.int32, (length, length), 1)
    lane = lax.broadcasted_iota(jnp.int32, (length, LANES), 1)
    lane_head = lax.broadcasted_iota(jnp.int32, (HEAD, LANES), 1)
    lower, upper = row >= col, row <= col
    queries = got[0, :, :LANES].astype(f32)
    queries = queries * jax.nn.sigmoid(queries)
    values = got[3, :, :LANES]
    pieces = []
    for j, mask in ((1, lower), (2, upper)):
        gate = got[j, :, :LANES].astype(f32)
        taken = gaps[j - 1 : j, :] * jax.nn.sigmoid(-gate)
        kept = jnp.log1p(-taken)
        gone = dot(mask.astype(f32), kept, ((1,), (0,)), lax.Precision.HIGHEST)
        total = gone[length - 1 : length] if j == 1 else gone[0:1]
        middle = gone[length // 2 : length // 2 + 1]
        decay = jnp.exp(total)
        state = dot(
            values, (taken * jnp.exp(total - gone)).astype(bf16), ((0,), (0,))
        )
        state = jnp.where(lane_head < HEAD, state[:HEAD], state[HEAD:])
        reader = read_fwd if j == 1 else read_bwd
        reader[...] = (queries * jnp.exp(gone)).astype(bf16)
        high = decay.astype(bf16)
        low = (decay - high.astype(f32)).astype(bf16)
        pieces.append((state.astype(bf16), high, low))
        query_part = queries * jnp.exp(gone - middle)
        key_part = (taken * jnp.exp(middle - gone)).astype(bf16)
        for h in range(2):
            inside = (lane >= h * HEAD) & (lane < (h + 1) * HEAD)
            score = dot(
                jnp.where(inside, query_part, 0.0).astype(bf16), key_part, ((1,), (1,))
            )
            pieces.append(jnp.where(mask, score, 0.0))
    (fwd, fwd_0, fwd_1, bwd, bwd_0, bwd_1) = pieces
    out_0 = dot((fwd_0 + bwd_0).astype(bf16), values, ((1,), (0,)))
    out_1 = dot((fwd_1 + bwd_1).astype(bf16), values, ((1,), (0,)))
    local[...] = jnp.where(lane < HEAD, out_0, out_1)
    keys_values = jnp.where(lane < HEAD, got[1, :, LANES:], got[2, :, LANES:])
    spare = STATE_ROWS - HEAD
    row_spare = lax.broadcasted_iota(jnp.int32, (spare, LANES), 0)

    def tail(piece):
        high = jnp.broadcast_to(piece[1].astype(f32), (spare, LANES))
        low = jnp.broadcast_to(piece[2].astype(f32), (spare, LANES))
        return jnp.where(row_spare == 0, high, low).astype(bf16)

    tails = tail(fwd), tail(bwd)
    for d in range(devices):
        message[d, :length] = keys_values

        @pl.when(d > me)
        def _():
            message[d, length : length + HEAD] = fwd[0]
            message[d, length + HEAD :] = tails[0]

        @pl.when(d <= me)
        def _():
            message[d, length : length + HEAD] = bwd[0]
            message[d, length + HEAD :] = tails[1]


def finish_kernel(
    place, lam, got, df_query, local, read_fwd, read_bwd, hg_gain, df_gain, hg_w, df_w, out, mixed
):
    devices = got.shape[0]
    length = local.shape[0]
    me = place[0]
    lane = lax.broadcasted_iota(jnp.int32, (length, LANES), 1)

    def folded(order, passed):
        state = jnp.zeros((HEAD, LANES), f32)
        for w in order:
            fresh = got[w, length : length + HEAD].astype(f32)
            tail = got[w, length + HEAD :].astype(f32)
            decay = tail[0:1] + tail[1:2]
            state = jnp.where(passed(w), decay * state + fresh, state)
        return state.astype(bf16)

    fwd = folded(range(devices), lambda w: w < me)
    bwd = folded(range(devices - 1, -1, -1), lambda w: w > me)
    recurrent = local[...]
    parts = []
    for h in range(2):
        inside = (lane >= h * HEAD) & (lane < (h + 1) * HEAD)
        zero = jnp.zeros((length, LANES), bf16)
        parts.append(
            dot(jnp.where(inside, read_fwd[...], zero), fwd, ((1,), (1,)))
            + dot(jnp.where(inside, read_bwd[...], zero), bwd, ((1,), (1,)))
        )
    recurrent = recurrent + jnp.concatenate(parts, axis=1)
    squares = recurrent * recurrent
    first = jnp.sum(jnp.where(lane < HEAD, squares, 0.0), axis=1, keepdims=True)
    second = jnp.sum(jnp.where(lane < HEAD, 0.0, squares), axis=1, keepdims=True)
    mean = jnp.where(lane < HEAD, first, second) * (1.0 / HEAD)
    mixed[:, :LANES] = (recurrent * lax.rsqrt(mean + epsilon) * hg_gain[...]).astype(bf16)

    step = 64
    keys_values = got[:, :length, :].reshape(devices * length, LANES)
    lane_step = lax.broadcasted_iota(jnp.int32, (step, LANES), 1)
    lam_value = lam[0]

    def attend(i, carry):
        rows = pl.ds(pl.multiple_of(i * step, step), step)
        query = df_query[rows, :]
        maps = []
        for m in range(2):
            inside = (lane_step >= m * DQK) & (lane_step < (m + 1) * DQK)
            only = jnp.where(inside, query, jnp.zeros_like(query))
            scores = dot(only, keys_values, ((1,), (1,))) * (DQK ** (-0.5))
            shifted = jnp.exp(scores - jnp.max(scores, axis=-1, keepdims=True))
            totals = jnp.sum(shifted, axis=-1, keepdims=True)
            maps.append(dot(shifted.astype(bf16), keys_values, ((1,), (0,))) / totals)
        weighted = (maps[0] - lam_value * maps[1])[:, HEAD:]
        mean = jnp.mean(weighted * weighted, axis=-1, keepdims=True)
        normed = (weighted * lax.rsqrt(mean + epsilon) * df_gain[...] * df_factor).astype(bf16)
        mixed[rows, LANES : LANES + HEAD] = normed
        return carry

    lax.fori_loop(0, length // step, attend, 0)
    out[...] = (
        dot(mixed[:, :LANES], hg_w[...], ((1,), (0,)))
        + dot(mixed[:, LANES : LANES + HEAD], df_w[...], ((1,), (0,)))
    ).astype(bf16)


def close_kernel(parts, gain, out):
    mixture = parts[0].astype(f32)
    for k in range(1, parts.shape[0]):
        mixture = mixture + parts[k].astype(f32)
    scale = lax.rsqrt(jnp.mean(mixture * mixture, axis=-1, keepdims=True) + epsilon)
    out[0] = (mixture * scale * gain[...]).astype(bf16)


def shards(
    inputs,
    norm_gain,
    hg_query_w,
    hg_fwd_w,
    hg_bwd_w,
    hg_value_w,
    floor_gap,
    hg_norm_gain,
    df_query_w,
    df_key_w,
    df_value_w,
    diff_lambda,
    df_norm_gain,
    out_hg_w,
    out_df_w,
    post_gain,
):
    sp, fs, tp = (lax.axis_size(a) for a in ("sp", "fs", "tp"))
    z, y = lax.axis_index("sp"), lax.axis_index("fs")
    _, length, width = inputs.shape
    depth = hg_query_w.shape[0]
    packed = depth + depth // 2

    sent = pl.pallas_call(
        pack_kernel,
        out_shape=jax.ShapeDtypeStruct((sp, fs, packed, LANES), bf16),
        name="pack",
    )(hg_query_w, hg_fwd_w, hg_bwd_w, hg_value_w, df_query_w, df_key_w, df_value_w)
    weights = lax.all_to_all(
        sent.reshape(sp * fs, packed, LANES), ("sp", "fs"), 0, 0, tiled=True
    )

    normed = pl.pallas_call(
        norm_kernel,
        out_shape=jax.ShapeDtypeStruct((length, width), bf16),
        name="norm",
    )(inputs, norm_gain[None])

    def shifted(array, by):
        return lax.ppermute(array, "fs", [(i, (i + by) % fs) for i in range(fs)])

    before = shifted(normed, 1)
    after = shifted(normed, -1)
    far_top = shifted(before[: length // 2], 1)
    far_low = shifted(after[length // 2 :], -1)
    places = jnp.stack([y, (y + fs - 1) % fs, (y + 1) % fs, (y + 2) % fs]).astype(jnp.int32)
    vmem = pl.BlockSpec(memory_space=pltpu.VMEM)
    projected = pl.pallas_call(
        project_kernel,
        in_specs=[SMEM_SPEC] + [vmem] * 6,
        out_specs=vmem,
        out_shape=jax.ShapeDtypeStruct((fs, length, 2 * LANES), bf16),
        scratch_shapes=[pltpu.VMEM((width, 2 * LANES), bf16)],
        name="project",
    )(places, normed, before, after, far_top, far_low, weights)
    got = lax.all_to_all(projected, "fs", 0, 0, tiled=True)

    place = z.astype(jnp.int32)[None]
    message, local, read_fwd, read_bwd = pl.pallas_call(
        local_kernel,
        in_specs=[SMEM_SPEC] + [vmem] * 2,
        out_specs=[vmem] * 4,
        out_shape=[
            jax.ShapeDtypeStruct((sp, length + STATE_ROWS, LANES), bf16),
            jax.ShapeDtypeStruct((length, LANES), f32),
            jax.ShapeDtypeStruct((length, LANES), bf16),
            jax.ShapeDtypeStruct((length, LANES), bf16),
        ],
        name="local",
    )(place, got, floor_gap)
    arrived = lax.all_to_all(message, "sp", 0, 0, tiled=True)
    partial = pl.pallas_call(
        finish_kernel,
        in_specs=[SMEM_SPEC] * 2 + [vmem] * 9,
        out_specs=vmem,
        out_shape=jax.ShapeDtypeStruct((length, width), bf16),
        scratch_shapes=[pltpu.VMEM((length, 2 * LANES), bf16)],
        name="finish",
    )(
        place,
        diff_lambda,
        arrived,
        got[0, :, LANES:],
        local,
        read_fwd,
        read_bwd,
        jnp.concatenate([hg_norm_gain, hg_norm_gain])[None],
        df_norm_gain[None],
        out_hg_w,
        out_df_w,
    )
    parts = lax.all_to_all(
        partial.reshape(tp, length // tp, width), "tp", 0, 0, tiled=True
    )
    return pl.pallas_call(
        close_kernel,
        out_shape=jax.ShapeDtypeStruct((1, length // tp, width), bf16),
        name="close",
    )(parts, post_gain[None])


def solution(mesh):
    rows = P(("sp", "fs"), "tp")
    in_specs = (
        P("fs", "sp", None),
        P(),
        rows,
        rows,
        rows,
        rows,
        P(None, "tp"),
        P(),
        rows,
        rows,
        rows,
        P("tp"),
        P(),
        P("tp", None),
        P("tp", None),
        P(),
    )
    out_specs = P("fs", ("sp", "tp"), None)
    return jax.shard_map(shards, mesh=mesh, in_specs=in_specs, out_specs=out_specs, check_vma=False)
```

```python
import jax
import jax.numpy as jnp
from jax import lax
from jax.experimental import pallas as pl
from jax.experimental.pallas import tpu as pltpu
from jax.sharding import PartitionSpec as P

HEAD = 64
DQK = 32
LANES = 128
STATE_ROWS = 72

epsilon = 1e-06
df_factor = 0.8
f32 = jnp.float32
bf16 = jnp.bfloat16

SMEM_SPEC = pl.BlockSpec(memory_space=pltpu.SMEM)
VMEM_SPEC = pl.BlockSpec(memory_space=pltpu.VMEM)
LIMIT = pltpu.CompilerParams(vmem_limit_bytes=24 * 2**20)


FAR_SPEC = pl.BlockSpec(memory_space=pltpu.HBM)


def there(array):
    return pltpu.with_memory_space_constraint(array, pltpu.HBM)


def here(array):
    return pltpu.with_memory_space_constraint(array, pltpu.VMEM)


def dot(a, b, dims, precision=None):
    return lax.dot_general(a, b, (dims, ((), ())), precision=precision, preferred_element_type=f32)


def pack_kernel(q, f, b, v, dq, dk, dv, out, wide, narrow, sems):
    copies = [
        pltpu.make_async_copy(source, wide.at[j], sems.at[j])
        for j, source in enumerate((q, f, b, v))
    ] + [
        pltpu.make_async_copy(source, narrow.at[j], sems.at[4 + j])
        for j, source in enumerate((dq, dk, dv))
    ]
    for copy in copies:
        copy.start()
    for copy in copies:
        copy.wait()
    half = q.shape[0] // 2
    for j in range(4):
        k = j % 3
        folded = jnp.concatenate([narrow[k, :half, :], narrow[k, half:, :]], axis=1)
        out[j] = jnp.concatenate([wide[j], folded], axis=0)


def norm_kernel(x, gain, out):
    rows = x[0].astype(f32)
    scale = lax.rsqrt(jnp.mean(rows * rows, axis=-1, keepdims=True) + epsilon)
    done = (rows * scale * gain[...]).astype(bf16)
    for k in range(out.shape[0]):
        out[k] = done


def project_kernel(rows, weights, out, rhs):
    blocks, packed, _ = weights.shape
    depth = packed * 2 // 3
    wide = weights[:, :depth, :]
    narrow = weights[:, depth:, :].astype(f32)
    first, second = narrow[:, :, :HEAD], narrow[:, :, HEAD:]
    narrow = jnp.concatenate(
        [
            jnp.concatenate([first, first], axis=2),
            jnp.concatenate([second, second], axis=2),
        ],
        axis=1,
    ).astype(bf16)
    rhs[:, :LANES] = wide.reshape(blocks * depth, LANES)
    rhs[:, LANES:] = narrow.reshape(blocks * depth, LANES)
    for k in range(rows.shape[0]):
        out[k] = dot(rows[k], rhs[...], ((1,), (0,))).astype(bf16)


def local_kernel(place, got, gaps, gains_in, message, local, read_fwd, read_bwd, gains):
    gains[...] = gains_in[...]
    length = got.shape[1]
    devices = message.shape[0]
    me = place[0]
    row = lax.broadcasted_iota(jnp.int32, (length, length), 0)
    col = lax.broadcasted_iota(jnp.int32, (length, length), 1)
    lane = lax.broadcasted_iota(jnp.int32, (length, LANES), 1)
    lane_head = lax.broadcasted_iota(jnp.int32, (HEAD, LANES), 1)
    lower, upper = row >= col, row <= col
    queries = got[0, :, :LANES].astype(f32)
    queries = queries * jax.nn.sigmoid(queries)
    values = got[3, :, :LANES]
    pieces = []
    for j, mask in ((1, lower), (2, upper)):
        gate = got[j, :, :LANES].astype(f32)
        taken = gaps[j - 1 : j, :] * jax.nn.sigmoid(-gate)
        kept = jnp.log1p(-taken)
        gone = dot(mask.astype(f32), kept, ((1,), (0,)), lax.Precision.HIGHEST)
        total = gone[length - 1 : length] if j == 1 else gone[0:1]
        middle = gone[length // 2 : length // 2 + 1]
        decay = jnp.exp(total)
        state = dot(
            values, (taken * jnp.exp(total - gone)).astype(bf16), ((0,), (0,))
        )
        state = jnp.where(lane_head < HEAD, state[:HEAD], state[HEAD:])
        reader = read_fwd if j == 1 else read_bwd
        reader[...] = (queries * jnp.exp(gone)).astype(bf16)
        high = decay.astype(bf16)
        low = (decay - high.astype(f32)).astype(bf16)
        pieces.append((state.astype(bf16), high, low))
        query_part = queries * jnp.exp(gone - middle)
        key_part = (taken * jnp.exp(middle - gone)).astype(bf16)
        for h in range(2):
            inside = (lane >= h * HEAD) & (lane < (h + 1) * HEAD)
            score = dot(
                jnp.where(inside, query_part, 0.0).astype(bf16), key_part, ((1,), (1,))
            )
            pieces.append(jnp.where(mask, score, 0.0))
    (fwd, fwd_0, fwd_1, bwd, bwd_0, bwd_1) = pieces
    out_0 = dot((fwd_0 + bwd_0).astype(bf16), values, ((1,), (0,)))
    out_1 = dot((fwd_1 + bwd_1).astype(bf16), values, ((1,), (0,)))
    local[...] = jnp.where(lane < HEAD, out_0, out_1)
    keys_values = jnp.where(lane < HEAD, got[1, :, LANES:], got[2, :, LANES:])
    spare = STATE_ROWS - HEAD
    row_spare = lax.broadcasted_iota(jnp.int32, (spare, LANES), 0)

    def tail(piece):
        high = jnp.broadcast_to(piece[1].astype(f32), (spare, LANES))
        low = jnp.broadcast_to(piece[2].astype(f32), (spare, LANES))
        return jnp.where(row_spare == 0, high, low).astype(bf16)

    tails = tail(fwd), tail(bwd)
    for d in range(devices):
        message[d, :length] = keys_values

        @pl.when(d > me)
        def _():
            message[d, length : length + HEAD] = fwd[0]
            message[d, length + HEAD :] = tails[0]

        @pl.when(d <= me)
        def _():
            message[d, length : length + HEAD] = bwd[0]
            message[d, length + HEAD :] = tails[1]


def finish_kernel(
    place, lam, got, df_query, local, read_fwd, read_bwd, gains, hg_w, df_w, out, mixed
):
    devices = got.shape[0]
    length = local.shape[0]
    me = place[0]
    lane = lax.broadcasted_iota(jnp.int32, (length, LANES), 1)

    def folded(order, passed):
        state = jnp.zeros((HEAD, LANES), f32)
        for w in order:
            fresh = got[w, length : length + HEAD].astype(f32)
            tail = got[w, length + HEAD :].astype(f32)
            decay = tail[0:1] + tail[1:2]
            state = jnp.where(passed(w), decay * state + fresh, state)
        return state.astype(bf16)

    fwd = folded(range(devices), lambda w: w < me)
    bwd = folded(range(devices - 1, -1, -1), lambda w: w > me)
    recurrent = local[...]
    parts = []
    for h in range(2):
        inside = (lane >= h * HEAD) & (lane < (h + 1) * HEAD)
        zero = jnp.zeros((length, LANES), bf16)
        parts.append(
            dot(jnp.where(inside, read_fwd[...], zero), fwd, ((1,), (1,)))
            + dot(jnp.where(inside, read_bwd[...], zero), bwd, ((1,), (1,)))
        )
    recurrent = recurrent + jnp.concatenate(parts, axis=1)
    squares = recurrent * recurrent
    first = jnp.sum(jnp.where(lane < HEAD, squares, 0.0), axis=1, keepdims=True)
    second = jnp.sum(jnp.where(lane < HEAD, 0.0, squares), axis=1, keepdims=True)
    mean = jnp.where(lane < HEAD, first, second) * (1.0 / HEAD)
    mixed[:, :LANES] = (recurrent * lax.rsqrt(mean + epsilon) * gains[0:1]).astype(bf16)

    step = 64
    keys_values = got[:, :length, :].reshape(devices * length, LANES)
    lane_step = lax.broadcasted_iota(jnp.int32, (step, LANES), 1)
    lam_value = lam[0]

    def attend(i, carry):
        rows = pl.ds(pl.multiple_of(i * step, step), step)
        query = df_query[0, rows, LANES:]
        maps = []
        for m in range(2):
            inside = (lane_step >= m * DQK) & (lane_step < (m + 1) * DQK)
            only = jnp.where(inside, query, jnp.zeros_like(query))
            scores = dot(only, keys_values, ((1,), (1,))) * (DQK ** (-0.5))
            shifted = jnp.exp(scores - jnp.max(scores, axis=-1, keepdims=True))
            totals = jnp.sum(shifted, axis=-1, keepdims=True)
            maps.append(dot(shifted.astype(bf16), keys_values, ((1,), (0,))) / totals)
        weighted = (maps[0] - lam_value * maps[1])[:, HEAD:]
        mean = jnp.mean(weighted * weighted, axis=-1, keepdims=True)
        normed = (weighted * lax.rsqrt(mean + epsilon) * gains[1:2, :HEAD] * df_factor).astype(bf16)
        mixed[rows, LANES : LANES + HEAD] = normed
        return carry

    lax.fori_loop(0, length // step, attend, 0)
    out[...] = (
        dot(mixed[:, :LANES], hg_w[...], ((1,), (0,)))
        + dot(mixed[:, LANES : LANES + HEAD], df_w[...], ((1,), (0,)))
    ).astype(bf16)


def close_kernel(parts, gain, out):
    mixture = parts[0].astype(f32)
    for k in range(1, parts.shape[0]):
        mixture = mixture + parts[k].astype(f32)
    scale = lax.rsqrt(jnp.mean(mixture * mixture, axis=-1, keepdims=True) + epsilon)
    out[0] = (mixture * scale * gain[...]).astype(bf16)


def shards(
    inputs,
    norm_gain,
    hg_query_w,
    hg_fwd_w,
    hg_bwd_w,
    hg_value_w,
    floor_gap,
    hg_norm_gain,
    df_query_w,
    df_key_w,
    df_value_w,
    diff_lambda,
    df_norm_gain,
    out_hg_w,
    out_df_w,
    post_gain,
):
    sp, fs, tp = (lax.axis_size(a) for a in ("sp", "fs", "tp"))
    z = lax.axis_index("sp")
    _, length, width = inputs.shape
    depth = hg_query_w.shape[0]
    packed = depth + depth // 2

    vmem = VMEM_SPEC
    normed = pl.pallas_call(
        norm_kernel,
        out_shape=pltpu.VMEM((fs, length, width), bf16),
        compiler_params=LIMIT,
        name="norm",
    )(inputs, norm_gain[None])

    rows = lax.all_to_all(normed, "fs", 0, 0, tiled=True)
    sources = (hg_query_w, hg_fwd_w, hg_bwd_w, hg_value_w, df_query_w, df_key_w, df_value_w)
    sent = pl.pallas_call(
        pack_kernel,
        in_specs=[FAR_SPEC] * 7,
        out_specs=vmem,
        out_shape=pltpu.VMEM((fs, packed, LANES), bf16),
        scratch_shapes=[
            pltpu.VMEM((4, depth, LANES), bf16),
            pltpu.VMEM((3, depth, LANES // 2), bf16),
            pltpu.SemaphoreType.DMA((7,)),
        ],
        compiler_params=LIMIT,
        name="pack",
    )(*map(there, sources))
    mine = lax.all_to_all(sent, "fs", 0, 0, tiled=True)
    weights = lax.all_gather(mine[None], "sp", axis=0, tiled=True)
    weights = weights.reshape(sp * fs, packed, LANES)
    projected = pl.pallas_call(
        project_kernel,
        in_specs=[vmem] * 2,
        out_specs=vmem,
        out_shape=pltpu.VMEM((fs, length, 2 * LANES), bf16),
        scratch_shapes=[pltpu.VMEM((width, 2 * LANES), bf16)],
        compiler_params=LIMIT,
        name="project",
    )(here(rows), here(weights))
    got = lax.all_to_all(projected, "fs", 0, 0, tiled=True)

    place = z.astype(jnp.int32)[None]
    gains = jnp.concatenate([hg_norm_gain, hg_norm_gain, df_norm_gain, df_norm_gain])
    message, local, read_fwd, read_bwd, gains = pl.pallas_call(
        local_kernel,
        in_specs=[SMEM_SPEC] + [vmem] * 3,
        out_specs=[vmem] * 5,
        out_shape=[
            pltpu.VMEM((sp, length + STATE_ROWS, LANES), bf16),
            pltpu.VMEM((length, LANES), f32),
            pltpu.VMEM((length, LANES), bf16),
            pltpu.VMEM((length, LANES), bf16),
            pltpu.VMEM((2, LANES), f32),
        ],
        compiler_params=LIMIT,
        name="local",
    )(place, here(got), here(floor_gap), here(gains.reshape(2, LANES)))
    arrived = lax.all_to_all(message, "sp", 0, 0, tiled=True)
    partial = pl.pallas_call(
        finish_kernel,
        in_specs=[SMEM_SPEC] * 2 + [vmem] * 8,
        out_specs=vmem,
        out_shape=pltpu.VMEM((length, width), bf16),
        scratch_shapes=[pltpu.VMEM((length, 2 * LANES), bf16)],
        compiler_params=LIMIT,
        name="finish",
    )(
        place,
        diff_lambda,
        here(arrived),
        here(got),
        here(local),
        here(read_fwd),
        here(read_bwd),
        here(gains),
        here(out_hg_w),
        here(out_df_w),
    )
    parts = lax.all_to_all(
        partial.reshape(tp, length // tp, width), "tp", 0, 0, tiled=True
    )
    return pl.pallas_call(
        close_kernel,
        out_shape=jax.ShapeDtypeStruct((1, length // tp, width), bf16),
        compiler_params=LIMIT,
        name="close",
    )(here(parts), post_gain[None])


def solution(mesh):
    rows = P(("sp", "fs"), "tp")
    in_specs = (
        P("fs", "sp", None),
        P(),
        rows,
        rows,
        rows,
        rows,
        P(None, "tp"),
        P(),
        rows,
        rows,
        rows,
        P("tp"),
        P(),
        P("tp", None),
        P("tp", None),
        P(),
    )
    out_specs = P("fs", ("sp", "tp"), None)
    return jax.shard_map(
        shards, mesh=mesh, in_specs=in_specs, out_specs=out_specs, check_vma=False
    )
```

```python
import jax
import jax.numpy as jnp
from jax import lax
from jax.experimental import pallas as pl
from jax.experimental.pallas import tpu as pltpu
from jax.sharding import PartitionSpec as P

HEAD = 64
DQK = 32
LANES = 128
EXTRA = 16
TAIL = 8

epsilon = 1e-06
df_factor = 0.8
f32 = jnp.float32
bf16 = jnp.bfloat16

SMEM_SPEC = pl.BlockSpec(memory_space=pltpu.SMEM)
VMEM_SPEC = pl.BlockSpec(memory_space=pltpu.VMEM)
LIMIT = pltpu.CompilerParams(vmem_limit_bytes=24 * 2**20)


FAR_SPEC = pl.BlockSpec(memory_space=pltpu.HBM)


def there(array):
    return pltpu.with_memory_space_constraint(array, pltpu.HBM)


def here(array):
    return pltpu.with_memory_space_constraint(array, pltpu.VMEM)


def dot(a, b, dims, precision=None):
    return lax.dot_general(a, b, (dims, ((), ())), precision=precision, preferred_element_type=f32)


def pack_kernel(q, f, b, v, dq, dk, dv, out, wide, narrow, sems):
    copies = [
        pltpu.make_async_copy(source, wide.at[j], sems.at[j])
        for j, source in enumerate((q, f, b, v))
    ] + [
        pltpu.make_async_copy(source, narrow.at[j], sems.at[4 + j])
        for j, source in enumerate((dq, dk, dv))
    ]
    for copy in copies:
        copy.start()
    for copy in copies:
        copy.wait()
    half = q.shape[0] // 2
    for j in range(4):
        k = j % 3
        folded = jnp.concatenate([narrow[k, :half, :], narrow[k, half:, :]], axis=1)
        out[j] = jnp.concatenate([wide[j], folded], axis=0)


def norm_kernel(x, gain, out):
    rows = x[0].astype(f32)
    scale = lax.rsqrt(jnp.mean(rows * rows, axis=-1, keepdims=True) + epsilon)
    done = (rows * scale * gain[...]).astype(bf16)
    for k in range(out.shape[0]):
        out[k] = done


def project_kernel(rows, weights, out, rhs):
    blocks, packed, _ = weights.shape
    depth = packed * 2 // 3
    wide = weights[:, :depth, :]
    narrow = weights[:, depth:, :].astype(f32)
    first, second = narrow[:, :, :HEAD], narrow[:, :, HEAD:]
    narrow = jnp.concatenate(
        [
            jnp.concatenate([first, first], axis=2),
            jnp.concatenate([second, second], axis=2),
        ],
        axis=1,
    ).astype(bf16)
    rhs[:, :LANES] = wide.reshape(blocks * depth, LANES)
    rhs[:, LANES:] = narrow.reshape(blocks * depth, LANES)
    for k in range(rows.shape[0]):
        out[k] = dot(rows[k], rhs[...], ((1,), (0,))).astype(bf16)


def local_kernel(got, gaps, gains_in, held, states, local, read_fwd, read_bwd, gains):
    gains[...] = gains_in[...]
    length = got.shape[1]
    row = lax.broadcasted_iota(jnp.int32, (length, length), 0)
    col = lax.broadcasted_iota(jnp.int32, (length, length), 1)
    lane = lax.broadcasted_iota(jnp.int32, (length, LANES), 1)
    lane_head = lax.broadcasted_iota(jnp.int32, (HEAD, LANES), 1)
    lower, upper = row >= col, row <= col
    queries = got[0, :, :LANES].astype(f32)
    queries = queries * jax.nn.sigmoid(queries)
    values = got[3, :, :LANES]
    pieces = []
    for j, mask in ((1, lower), (2, upper)):
        gate = got[j, :, :LANES].astype(f32)
        taken = gaps[j - 1 : j, :] * jax.nn.sigmoid(-gate)
        kept = jnp.log1p(-taken)
        gone = dot(mask.astype(f32), kept, ((1,), (0,)), lax.Precision.HIGHEST)
        total = gone[length - 1 : length] if j == 1 else gone[0:1]
        middle = gone[length // 2 : length // 2 + 1]
        decay = jnp.exp(total)
        state = dot(
            values, (taken * jnp.exp(total - gone)).astype(bf16), ((0,), (0,))
        )
        state = jnp.where(lane_head < HEAD, state[:HEAD], state[HEAD:])
        reader = read_fwd if j == 1 else read_bwd
        reader[...] = (queries * jnp.exp(gone)).astype(bf16)
        high = decay.astype(bf16)
        low = (decay - high.astype(f32)).astype(bf16)
        pieces.append((state, high, low))
        query_part = queries * jnp.exp(gone - middle)
        key_part = (taken * jnp.exp(middle - gone)).astype(bf16)
        for h in range(2):
            inside = (lane >= h * HEAD) & (lane < (h + 1) * HEAD)
            score = dot(
                jnp.where(inside, query_part, 0.0).astype(bf16), key_part, ((1,), (1,))
            )
            pieces.append(jnp.where(mask, score, 0.0))
    (fwd, fwd_0, fwd_1, bwd, bwd_0, bwd_1) = pieces
    out_0 = dot((fwd_0 + bwd_0).astype(bf16), values, ((1,), (0,)))
    out_1 = dot((fwd_1 + bwd_1).astype(bf16), values, ((1,), (0,)))
    local[...] = jnp.where(lane < HEAD, out_0, out_1)
    held[...] = jnp.where(lane < HEAD, got[1, :, LANES:], got[2, :, LANES:])
    states[: 2 * HEAD] = jnp.concatenate([fwd[0], bwd[0]], axis=0).astype(bf16)
    states[2 * HEAD :] = stacked(EXTRA, (fwd[1], fwd[2], bwd[1], bwd[2]))


def stacked(count, lines):
    row = lax.broadcasted_iota(jnp.int32, (count, LANES), 0)
    block = jnp.zeros((count, LANES), f32)
    for k, line in enumerate(lines):
        block = jnp.where(row == k, jnp.broadcast_to(line.astype(f32), (count, LANES)), block)
    return block.astype(bf16)


def halves(value):
    high = value.astype(bf16)
    return high, (value - high.astype(f32)).astype(bf16)


def pair_kernel(place, held, mine, other, out):
    length = held.shape[0]
    odd = lax.rem(place[0], 2) == 1
    mine_all = mine[: 2 * HEAD].astype(f32)
    other_all = other[: 2 * HEAD].astype(f32)
    low = jnp.where(odd, other_all, mine_all)
    high = jnp.where(odd, mine_all, other_all)
    mine_tail = mine[2 * HEAD :].astype(f32)
    other_tail = other[2 * HEAD :].astype(f32)
    low_tail = jnp.where(odd, other_tail, mine_tail)
    high_tail = jnp.where(odd, mine_tail, other_tail)
    low_fwd, low_bwd = low_tail[0:1] + low_tail[1:2], low_tail[2:3] + low_tail[3:4]
    high_fwd, high_bwd = high_tail[0:1] + high_tail[1:2], high_tail[2:3] + high_tail[3:4]
    fwd = high_fwd * low[:HEAD] + high[:HEAD]
    bwd = low_bwd * high[HEAD:] + low[HEAD:]
    half = HEAD // 2
    part = jnp.concatenate(
        [
            jnp.where(odd, fwd[half:], fwd[:half]),
            jnp.where(odd, bwd[half:], bwd[:half]),
        ],
        axis=0,
    )
    out[:length] = held[...]
    out[length : length + HEAD] = part.astype(bf16)
    lines = (*halves(low_fwd * high_fwd), *halves(low_bwd * high_bwd))
    out[length + HEAD :] = stacked(TAIL, lines)


def finish_kernel(
    place, lam, got, other, df_query, local, read_fwd, read_bwd, gains, hg_w, df_w, out,
    mixed, rows_w, sems
):
    devices = got.shape[0]
    length = local.shape[0]
    me = place[0]
    copies = [
        pltpu.make_async_copy(hg_w, rows_w.at[:LANES], sems.at[0]),
        pltpu.make_async_copy(df_w, rows_w.at[LANES:], sems.at[1]),
    ]
    for copy in copies:
        copy.start()
    lane = lax.broadcasted_iota(jnp.int32, (length, LANES), 1)

    half = HEAD // 2
    pair, odd = me // 2, lax.rem(me, 2) == 1
    partner = other[: 2 * HEAD].astype(f32)
    partner_tail = other[2 * HEAD :].astype(f32)

    def folded(order, passed, k):
        state = jnp.zeros((HEAD, LANES), f32)
        rows = slice(length + k * half, length + (k + 1) * half)
        for w in order:
            fresh = jnp.concatenate([got[2 * w, rows], got[2 * w + 1, rows]], axis=0).astype(f32)
            tail = got[2 * w, length + HEAD :].astype(f32)
            decay = tail[2 * k : 2 * k + 1] + tail[2 * k + 1 : 2 * k + 2]
            state = jnp.where(passed(w), decay * state + fresh, state)
        decay = partner_tail[2 * k : 2 * k + 1] + partner_tail[2 * k + 1 : 2 * k + 2]
        joined = decay * state + partner[k * HEAD : (k + 1) * HEAD]
        return jnp.where(odd if k == 0 else jnp.logical_not(odd), joined, state).astype(bf16)

    fwd = folded(range(devices // 2), lambda w: w < pair, 0)
    bwd = folded(range(devices // 2 - 1, -1, -1), lambda w: w > pair, 1)
    recurrent = local[...]
    parts = []
    for h in range(2):
        inside = (lane >= h * HEAD) & (lane < (h + 1) * HEAD)
        zero = jnp.zeros((length, LANES), bf16)
        parts.append(
            dot(jnp.where(inside, read_fwd[...], zero), fwd, ((1,), (1,)))
            + dot(jnp.where(inside, read_bwd[...], zero), bwd, ((1,), (1,)))
        )
    recurrent = recurrent + jnp.concatenate(parts, axis=1)
    squares = recurrent * recurrent
    first = jnp.sum(jnp.where(lane < HEAD, squares, 0.0), axis=1, keepdims=True)
    second = jnp.sum(jnp.where(lane < HEAD, 0.0, squares), axis=1, keepdims=True)
    mean = jnp.where(lane < HEAD, first, second) * (1.0 / HEAD)
    mixed[:, :LANES] = (recurrent * lax.rsqrt(mean + epsilon) * gains[0:1]).astype(bf16)

    keys_values = got[:, :length, :].reshape(devices * length, LANES)
    query = df_query[0, :, LANES:]
    only = jnp.concatenate(
        [
            jnp.where((lane >= m * DQK) & (lane < (m + 1) * DQK), query, jnp.zeros_like(query))
            for m in range(2)
        ],
        axis=0,
    )
    scores = dot(only, keys_values, ((1,), (1,))) * (DQK ** (-0.5))
    shifted = jnp.exp(scores - jnp.max(scores, axis=-1, keepdims=True))
    totals = jnp.sum(shifted, axis=-1, keepdims=True)
    maps = dot(shifted.astype(bf16), keys_values, ((1,), (0,))) / totals
    weighted = (maps[:length] - lam[0] * maps[length:])[:, HEAD:]
    mean = jnp.mean(weighted * weighted, axis=-1, keepdims=True)
    mixed[:, LANES:] = (
        weighted * lax.rsqrt(mean + epsilon) * gains[1:2, :HEAD] * df_factor
    ).astype(bf16)
    for copy in copies:
        copy.wait()
    out[...] = dot(mixed[...], rows_w[...], ((1,), (0,))).astype(bf16)


def close_kernel(parts, gain, out):
    mixture = parts[0].astype(f32)
    for k in range(1, parts.shape[0]):
        mixture = mixture + parts[k].astype(f32)
    scale = lax.rsqrt(jnp.mean(mixture * mixture, axis=-1, keepdims=True) + epsilon)
    out[0] = (mixture * scale * gain[...]).astype(bf16)


def shards(
    inputs,
    norm_gain,
    hg_query_w,
    hg_fwd_w,
    hg_bwd_w,
    hg_value_w,
    floor_gap,
    hg_norm_gain,
    df_query_w,
    df_key_w,
    df_value_w,
    diff_lambda,
    df_norm_gain,
    out_hg_w,
    out_df_w,
    post_gain,
):
    sp, fs, tp = (lax.axis_size(a) for a in ("sp", "fs", "tp"))
    z = lax.axis_index("sp")
    _, length, width = inputs.shape
    depth = hg_query_w.shape[0]
    packed = depth + depth // 2

    vmem = VMEM_SPEC
    normed = pl.pallas_call(
        norm_kernel,
        out_shape=pltpu.VMEM((fs, length, width), bf16),
        compiler_params=LIMIT,
        name="norm",
    )(inputs, norm_gain[None])

    rows = lax.all_to_all(normed, "fs", 0, 0, tiled=True)
    sources = (hg_query_w, hg_fwd_w, hg_bwd_w, hg_value_w, df_query_w, df_key_w, df_value_w)
    sent = pl.pallas_call(
        pack_kernel,
        in_specs=[FAR_SPEC] * 7,
        out_specs=vmem,
        out_shape=pltpu.VMEM((fs, packed, LANES), bf16),
        scratch_shapes=[
            pltpu.VMEM((4, depth, LANES), bf16),
            pltpu.VMEM((3, depth, LANES // 2), bf16),
            pltpu.SemaphoreType.DMA((7,)),
        ],
        compiler_params=LIMIT,
        name="pack",
    )(*map(there, sources))
    mine = lax.all_to_all(sent, "fs", 0, 0, tiled=True)
    weights = lax.all_gather(mine[None], "sp", axis=0, tiled=True)
    weights = weights.reshape(sp * fs, packed, LANES)
    projected = pl.pallas_call(
        project_kernel,
        in_specs=[vmem] * 2,
        out_specs=vmem,
        out_shape=pltpu.VMEM((fs, length, 2 * LANES), bf16),
        scratch_shapes=[pltpu.VMEM((width, 2 * LANES), bf16)],
        compiler_params=LIMIT,
        name="project",
    )(here(rows), here(weights))
    got = lax.all_to_all(projected, "fs", 0, 0, tiled=True)

    place = z.astype(jnp.int32)[None]
    gains = jnp.concatenate([hg_norm_gain, hg_norm_gain, df_norm_gain, df_norm_gain])
    held, states, local, read_fwd, read_bwd, gains = pl.pallas_call(
        local_kernel,
        in_specs=[vmem] * 3,
        out_specs=[vmem] * 6,
        out_shape=[
            pltpu.VMEM((length, LANES), bf16),
            pltpu.VMEM((2 * HEAD + EXTRA, LANES), bf16),
            pltpu.VMEM((length, LANES), f32),
            pltpu.VMEM((length, LANES), bf16),
            pltpu.VMEM((length, LANES), bf16),
            pltpu.VMEM((2, LANES), f32),
        ],
        compiler_params=LIMIT,
        name="local",
    )(here(got), here(floor_gap), here(gains.reshape(2, LANES)))
    other = lax.ppermute(states, "sp", [(i, i ^ 1) for i in range(sp)])
    joined = pl.pallas_call(
        pair_kernel,
        in_specs=[SMEM_SPEC] + [vmem] * 3,
        out_specs=vmem,
        out_shape=pltpu.VMEM((length + HEAD + TAIL, LANES), bf16),
        compiler_params=LIMIT,
        name="pair",
    )(place, here(held), here(states), here(other))
    arrived = lax.all_gather(joined[None], "sp", axis=0, tiled=True)
    partial = pl.pallas_call(
        finish_kernel,
        in_specs=[SMEM_SPEC] * 2 + [vmem] * 7 + [FAR_SPEC] * 2,
        out_specs=vmem,
        out_shape=pltpu.VMEM((length, width), bf16),
        scratch_shapes=[
            pltpu.VMEM((length, LANES + HEAD), bf16),
            pltpu.VMEM((LANES + HEAD, width), bf16),
            pltpu.SemaphoreType.DMA((2,)),
        ],
        compiler_params=LIMIT,
        name="finish",
    )(
        place,
        diff_lambda,
        here(arrived),
        here(other),
        here(got),
        here(local),
        here(read_fwd),
        here(read_bwd),
        here(gains),
        there(out_hg_w),
        there(out_df_w),
    )
    parts = lax.all_to_all(
        partial.reshape(tp, length // tp, width), "tp", 0, 0, tiled=True
    )
    return pl.pallas_call(
        close_kernel,
        out_shape=jax.ShapeDtypeStruct((1, length // tp, width), bf16),
        compiler_params=LIMIT,
        name="close",
    )(here(parts), post_gain[None])


def solution(mesh):
    rows = P(("sp", "fs"), "tp")
    in_specs = (
        P("fs", "sp", None),
        P(),
        rows,
        rows,
        rows,
        rows,
        P(None, "tp"),
        P(),
        rows,
        rows,
        rows,
        P("tp"),
        P(),
        P("tp", None),
        P("tp", None),
        P(),
    )
    out_specs = P("fs", ("sp", "tp"), None)
    return jax.shard_map(
        shards, mesh=mesh, in_specs=in_specs, out_specs=out_specs, check_vma=False
    )
```

```python
import jax
import jax.numpy as jnp
from jax import lax
from jax.experimental import pallas as pl
from jax.experimental.pallas import tpu as pltpu
from jax.sharding import PartitionSpec as P

HEAD = 64
DQK = 32
LANES = 128
TAIL = 8

epsilon = 1e-06
df_factor = 0.8
f32 = jnp.float32
bf16 = jnp.bfloat16

SMEM_SPEC = pl.BlockSpec(memory_space=pltpu.SMEM)
VMEM_SPEC = pl.BlockSpec(memory_space=pltpu.VMEM)
LIMIT = pltpu.CompilerParams(vmem_limit_bytes=24 * 2**20)


FAR_SPEC = pl.BlockSpec(memory_space=pltpu.HBM)


def there(array):
    return pltpu.with_memory_space_constraint(array, pltpu.HBM)


def here(array):
    return pltpu.with_memory_space_constraint(array, pltpu.VMEM)


def dot(a, b, dims, precision=None):
    return lax.dot_general(a, b, (dims, ((), ())), precision=precision, preferred_element_type=f32)


def pack_kernel(q, f, b, v, dq, dk, dv, out, wide, narrow, sems):
    copies = [
        pltpu.make_async_copy(source, wide.at[j], sems.at[j])
        for j, source in enumerate((q, f, b, v))
    ] + [
        pltpu.make_async_copy(source, narrow.at[j], sems.at[4 + j])
        for j, source in enumerate((dq, dk, dv))
    ]
    for copy in copies:
        copy.start()
    for copy in copies:
        copy.wait()
    half = q.shape[0] // 2
    for j in range(4):
        k = j % 3
        folded = jnp.concatenate([narrow[k, :half, :], narrow[k, half:, :]], axis=1)
        out[j] = jnp.concatenate([wide[j], folded], axis=0)


def norm_kernel(x, gain_in, out, rows, gain, sems):
    copies = (
        pltpu.make_async_copy(x.at[0], rows, sems.at[0]),
        pltpu.make_async_copy(gain_in, gain, sems.at[1]),
    )
    for copy in copies:
        copy.start()
    for copy in copies:
        copy.wait()
    part = rows[...].astype(f32)
    scale = lax.rsqrt(jnp.mean(part * part, axis=-1, keepdims=True) + epsilon)
    done = (part * scale * gain[...]).astype(bf16)
    for k in range(out.shape[0]):
        out[k] = done


def project_kernel(place, rows, weights, out, rhs):
    blocks, packed, _ = weights.shape
    depth = packed * 2 // 3
    half = depth // 2
    wide = weights[:, :depth, :]
    narrow = weights[:, depth:, :].astype(f32)
    first, second = narrow[:, :, :HEAD], narrow[:, :, HEAD:]
    narrow = jnp.concatenate(
        [
            jnp.concatenate([first, first], axis=2),
            jnp.concatenate([second, second], axis=2),
        ],
        axis=1,
    ).astype(bf16)
    rhs[:, :LANES] = wide.reshape(blocks * depth, LANES)
    rhs[:, LANES:] = narrow.reshape(blocks * depth, LANES)
    count, length, width = rows.shape
    whole = dot(rows[...].reshape(count * length, width), rhs[...], ((1,), (0,))).astype(bf16)
    half = length // 2
    lane = lax.broadcasted_iota(jnp.int32, (half, LANES), 1)
    turned = jnp.where(place[0] == 2, HEAD, 0)
    early = lax.rem(lane + turned, LANES) < HEAD
    for k in range(count):
        part = whole[k * length : (k + 1) * length]
        folded = jnp.where(early, part[:half, LANES:], part[half:, LANES:])
        for a in range(2):
            out[a, k, :length] = part[:, :LANES]
            out[a, k, length:] = folded


def swapped(block):
    return jnp.concatenate([block[:, HEAD:], block[:, :HEAD]], axis=1)


def local_kernel(
    place, got, gaps, gains_in, out, other, query_out, local, read_fwd, read_bwd, gains
):
    gains[...] = gains_in[...]
    length = local.shape[0]
    half = length // 2
    odd = place[0] == 1
    mine = place[0] * 4
    row = lax.broadcasted_iota(jnp.int32, (length, length), 0)
    col = lax.broadcasted_iota(jnp.int32, (length, length), 1)
    lane = lax.broadcasted_iota(jnp.int32, (length, LANES), 1)
    lane_head = lax.broadcasted_iota(jnp.int32, (HEAD, LANES), 1)
    masks = row >= col, row <= col
    takens, gones, states, decays = ({}, {}, {}, {})
    for slot in range(2):
        values = got[4 * slot + 3, :length]
        for d in range(2):
            gate = got[4 * slot + 1 + d, :length].astype(f32)
            taken = gaps[d : d + 1, :] * jax.nn.sigmoid(-gate)
            kept = jnp.log1p(-taken)
            gone = dot(masks[d].astype(f32), kept, ((1,), (0,)), lax.Precision.HIGHEST)
            total = gone[length - 1 : length] if d == 0 else gone[0:1]
            state = dot(values, (taken * jnp.exp(total - gone)).astype(bf16), ((0,), (0,)))
            takens[slot, d], gones[slot, d] = taken, gone
            states[slot, d] = jnp.where(lane_head < HEAD, state[:HEAD], state[HEAD:])
            decays[slot, d] = jnp.exp(total)
    fwd = decays[1, 0] * states[0, 0] + states[1, 0]
    bwd = decays[0, 1] * states[1, 1] + states[0, 1]
    quarter = HEAD // 2
    part = jnp.concatenate(
        [
            jnp.where(odd, fwd[quarter:], fwd[:quarter]),
            jnp.where(odd, bwd[quarter:], bwd[:quarter]),
        ],
        axis=0,
    )
    out[length : length + HEAD] = part.astype(bf16)
    lines = (*halves(decays[0, 0] * decays[1, 0]), *halves(decays[0, 1] * decays[1, 1]))
    out[length + HEAD :] = stacked(TAIL, lines)
    other[:HEAD] = states[0, 0]
    other[HEAD : 2 * HEAD] = states[1, 1]
    row_tail = lax.broadcasted_iota(jnp.int32, (TAIL, LANES), 0)
    other[2 * HEAD :] = jnp.where(row_tail == 0, decays[0, 0], decays[1, 1])

    keys, worth = got[mine + 1, length:], got[mine + 2, length:]
    lane_half = lane[:half]
    out[:half] = jnp.where(lane_half < HEAD, keys, worth)
    out[half:length] = swapped(jnp.where(lane_half < HEAD, worth, keys))
    folded = got[mine, length:]
    query_out[:half] = folded
    query_out[half:] = swapped(folded)

    queries = got[mine, :length].astype(f32)
    queries = queries * jax.nn.sigmoid(queries)
    values = got[mine + 3, :length]
    weights = [0.0, 0.0]
    for d in range(2):
        gone = jnp.where(odd, gones[1, d], gones[0, d])
        taken = jnp.where(odd, takens[1, d], takens[0, d])
        reader = read_bwd if d else read_fwd
        reader[...] = (queries * jnp.exp(gone)).astype(bf16)
        middle = gone[half : half + 1]
        query_part = queries * jnp.exp(gone - middle)
        key_part = (taken * jnp.exp(middle - gone)).astype(bf16)
        for h in range(2):
            inside = (lane >= h * HEAD) & (lane < (h + 1) * HEAD)
            score = dot(jnp.where(inside, query_part, 0.0).astype(bf16), key_part, ((1,), (1,)))
            weights[h] = weights[h] + jnp.where(masks[d], score, 0.0)
    out_0 = dot(weights[0].astype(bf16), values, ((1,), (0,)))
    out_1 = dot(weights[1].astype(bf16), values, ((1,), (0,)))
    local[...] = jnp.where(lane < HEAD, out_0, out_1)


def stacked(count, lines):
    row = lax.broadcasted_iota(jnp.int32, (count, LANES), 0)
    block = jnp.zeros((count, LANES), f32)
    for k, line in enumerate(lines):
        block = jnp.where(row == k, jnp.broadcast_to(line.astype(f32), (count, LANES)), block)
    return block.astype(bf16)


def halves(value):
    high = value.astype(bf16)
    return high, (value - high.astype(f32)).astype(bf16)


def finish_kernel(
    place, lam, got, other, df_query, local, read_fwd, read_bwd, gains, hg_w, df_w, out,
    mixed, rows_w, sems
):
    devices = got.shape[0]
    length = local.shape[0]
    me = place[0]
    copies = [
        pltpu.make_async_copy(hg_w, rows_w.at[:LANES], sems.at[0]),
        pltpu.make_async_copy(df_w, rows_w.at[LANES:], sems.at[1]),
    ]
    for copy in copies:
        copy.start()
    lane = lax.broadcasted_iota(jnp.int32, (length, LANES), 1)

    half = HEAD // 2
    pair, odd = me // 2, lax.rem(me, 2) == 1

    def folded(order, passed, k):
        state = jnp.zeros((HEAD, LANES), f32)
        rows = slice(length + k * half, length + (k + 1) * half)
        for w in order:
            fresh = jnp.concatenate([got[2 * w, rows], got[2 * w + 1, rows]], axis=0).astype(f32)
            tail = got[2 * w, length + HEAD :].astype(f32)
            decay = tail[2 * k : 2 * k + 1] + tail[2 * k + 1 : 2 * k + 2]
            state = jnp.where(passed(w), decay * state + fresh, state)
        decay = other[2 * HEAD + k : 2 * HEAD + k + 1]
        joined = decay * state + other[k * HEAD : (k + 1) * HEAD]
        return jnp.where(odd if k == 0 else jnp.logical_not(odd), joined, state).astype(bf16)

    fwd = folded(range(devices // 2), lambda w: w < pair, 0)
    bwd = folded(range(devices // 2 - 1, -1, -1), lambda w: w > pair, 1)
    recurrent = local[...]
    parts = []
    for h in range(2):
        inside = (lane >= h * HEAD) & (lane < (h + 1) * HEAD)
        zero = jnp.zeros((length, LANES), bf16)
        parts.append(
            dot(jnp.where(inside, read_fwd[...], zero), fwd, ((1,), (1,)))
            + dot(jnp.where(inside, read_bwd[...], zero), bwd, ((1,), (1,)))
        )
    recurrent = recurrent + jnp.concatenate(parts, axis=1)
    squares = recurrent * recurrent
    first = jnp.sum(jnp.where(lane < HEAD, squares, 0.0), axis=1, keepdims=True)
    second = jnp.sum(jnp.where(lane < HEAD, 0.0, squares), axis=1, keepdims=True)
    mean = jnp.where(lane < HEAD, first, second) * (1.0 / HEAD)
    mixed[:, :LANES] = (recurrent * lax.rsqrt(mean + epsilon) * gains[0:1]).astype(bf16)

    keys_values = got[:, :length, :].reshape(devices * length, LANES)
    query = df_query[...]
    only = jnp.concatenate(
        [
            jnp.where((lane >= m * DQK) & (lane < (m + 1) * DQK), query, jnp.zeros_like(query))
            for m in range(2)
        ],
        axis=0,
    )
    scores = dot(only, keys_values, ((1,), (1,))) * (DQK ** (-0.5))
    shifted = jnp.exp(scores - jnp.max(scores, axis=-1, keepdims=True))
    totals = jnp.sum(shifted, axis=-1, keepdims=True)
    maps = dot(shifted.astype(bf16), keys_values, ((1,), (0,))) / totals
    weighted = (maps[:length] - lam[0] * maps[length:])[:, HEAD:]
    mean = jnp.mean(weighted * weighted, axis=-1, keepdims=True)
    mixed[:, LANES:] = (
        weighted * lax.rsqrt(mean + epsilon) * gains[1:2, :HEAD] * df_factor
    ).astype(bf16)
    for copy in copies:
        copy.wait()
    out[...] = dot(mixed[...], rows_w[...], ((1,), (0,))).astype(bf16)


def close_kernel(parts, gain, out):
    mixture = parts[0].astype(f32)
    for k in range(1, parts.shape[0]):
        mixture = mixture + parts[k].astype(f32)
    scale = lax.rsqrt(jnp.mean(mixture * mixture, axis=-1, keepdims=True) + epsilon)
    out[0] = (mixture * scale * gain[...]).astype(bf16)


def shards(
    inputs,
    norm_gain,
    hg_query_w,
    hg_fwd_w,
    hg_bwd_w,
    hg_value_w,
    floor_gap,
    hg_norm_gain,
    df_query_w,
    df_key_w,
    df_value_w,
    diff_lambda,
    df_norm_gain,
    out_hg_w,
    out_df_w,
    post_gain,
):
    sp, fs, tp = (lax.axis_size(a) for a in ("sp", "fs", "tp"))
    z, y = lax.axis_index("sp"), lax.axis_index("fs")
    _, length, width = inputs.shape
    depth = hg_query_w.shape[0]
    packed = depth + depth // 2

    vmem = VMEM_SPEC
    normed = pl.pallas_call(
        norm_kernel,
        in_specs=[FAR_SPEC] * 2,
        out_specs=vmem,
        out_shape=pltpu.VMEM((fs, length, width), bf16),
        scratch_shapes=[
            pltpu.VMEM((length, width), bf16),
            pltpu.VMEM((1, width), f32),
            pltpu.SemaphoreType.DMA((2,)),
        ],
        compiler_params=LIMIT,
        name="norm",
    )(there(inputs), there(norm_gain[None]))
    rows = lax.all_to_all(normed, "fs", 0, 0, tiled=True)
    sources = (hg_query_w, hg_fwd_w, hg_bwd_w, hg_value_w, df_query_w, df_key_w, df_value_w)
    sent = pl.pallas_call(
        pack_kernel,
        in_specs=[FAR_SPEC] * 7,
        out_specs=vmem,
        out_shape=pltpu.VMEM((fs, packed, LANES), bf16),
        scratch_shapes=[
            pltpu.VMEM((4, depth, LANES), bf16),
            pltpu.VMEM((3, depth, LANES // 2), bf16),
            pltpu.SemaphoreType.DMA((7,)),
        ],
        compiler_params=LIMIT,
        name="pack",
    )(*map(there, sources))
    mine = lax.all_to_all(sent, "fs", 0, 0, tiled=True)
    weights = lax.all_gather(mine[None], "sp", axis=0, tiled=True)
    weights = weights.reshape(sp * fs, packed, LANES)
    projected = pl.pallas_call(
        project_kernel,
        in_specs=[SMEM_SPEC] + [vmem] * 2,
        out_specs=vmem,
        out_shape=pltpu.VMEM((2, fs, length + length // 2, LANES), bf16),
        scratch_shapes=[pltpu.VMEM((width, 2 * LANES), bf16)],
        compiler_params=LIMIT,
        name="project",
    )(y.astype(jnp.int32)[None], here(rows), here(weights))
    groups = [[2 * fs * i + k for k in range(2 * fs)] for i in range(sp // 2)]
    got = lax.all_to_all(
        projected.reshape(2 * fs, length + length // 2, LANES),
        ("sp", "fs"),
        0,
        0,
        axis_index_groups=groups,
        tiled=True,
    )

    place = z.astype(jnp.int32)[None]
    gains = jnp.concatenate([hg_norm_gain, hg_norm_gain, df_norm_gain, df_norm_gain])
    joined, other, query, local, read_fwd, read_bwd, gains = pl.pallas_call(
        local_kernel,
        in_specs=[SMEM_SPEC] + [vmem] * 3,
        out_specs=[vmem] * 7,
        out_shape=[
            pltpu.VMEM((length + HEAD + TAIL, LANES), bf16),
            pltpu.VMEM((2 * HEAD + TAIL, LANES), f32),
            pltpu.VMEM((length, LANES), bf16),
            pltpu.VMEM((length, LANES), f32),
            pltpu.VMEM((length, LANES), bf16),
            pltpu.VMEM((length, LANES), bf16),
            pltpu.VMEM((2, LANES), f32),
        ],
        compiler_params=LIMIT,
        name="local",
    )(place % 2, here(got), here(floor_gap), here(gains.reshape(2, LANES)))
    arrived = lax.all_gather(joined[None], "sp", axis=0, tiled=True)
    partial = pl.pallas_call(
        finish_kernel,
        in_specs=[SMEM_SPEC] * 2 + [vmem] * 7 + [FAR_SPEC] * 2,
        out_specs=vmem,
        out_shape=pltpu.VMEM((length, width), bf16),
        scratch_shapes=[
            pltpu.VMEM((length, LANES + HEAD), bf16),
            pltpu.VMEM((LANES + HEAD, width), bf16),
            pltpu.SemaphoreType.DMA((2,)),
        ],
        compiler_params=LIMIT,
        name="finish",
    )(
        place,
        diff_lambda,
        here(arrived),
        here(other),
        here(query),
        here(local),
        here(read_fwd),
        here(read_bwd),
        here(gains),
        there(out_hg_w),
        there(out_df_w),
    )
    parts = lax.all_to_all(
        partial.reshape(tp, length // tp, width), "tp", 0, 0, tiled=True
    )
    return pl.pallas_call(
        close_kernel,
        out_shape=jax.ShapeDtypeStruct((1, length // tp, width), bf16),
        compiler_params=LIMIT,
        name="close",
    )(here(parts), post_gain[None])


def solution(mesh):
    rows = P(("sp", "fs"), "tp")
    in_specs = (
        P("fs", "sp", None),
        P(),
        rows,
        rows,
        rows,
        rows,
        P(None, "tp"),
        P(),
        rows,
        rows,
        rows,
        P("tp"),
        P(),
        P("tp", None),
        P("tp", None),
        P(),
    )
    out_specs = P("fs", ("sp", "tp"), None)
    return jax.shard_map(shards, mesh=mesh, in_specs=in_specs, out_specs=out_specs, check_vma=False)
```

```python
import jax
import jax.numpy as jnp
from jax import lax
from jax.experimental import pallas as pl
from jax.experimental.pallas import tpu as pltpu
from jax.sharding import PartitionSpec as P

HEAD = 64
DQK = 32
LANES = 128
TAIL = 8
EXTRA = 16

epsilon = 1e-06
df_factor = 0.8
f32 = jnp.float32
bf16 = jnp.bfloat16

SMEM_SPEC = pl.BlockSpec(memory_space=pltpu.SMEM)
VMEM_SPEC = pl.BlockSpec(memory_space=pltpu.VMEM)
LIMIT = pltpu.CompilerParams(vmem_limit_bytes=24 * 2**20)


FAR_SPEC = pl.BlockSpec(memory_space=pltpu.HBM)


def there(array):
    return pltpu.with_memory_space_constraint(array, pltpu.HBM)


def here(array):
    return pltpu.with_memory_space_constraint(array, pltpu.VMEM)


def dot(a, b, dims, precision=None):
    return lax.dot_general(a, b, (dims, ((), ())), precision=precision, preferred_element_type=f32)


def thirds(value):
    pieces = []
    for _ in range(3):
        pieces.append(value.astype(bf16))
        value = value - pieces[-1].astype(f32)
    return pieces


def pack_kernel(lam, q, f, b, v, dq, dk, dv, gaps_in, out, wide, narrow, gaps, sems):
    copies = [
        pltpu.make_async_copy(source, wide.at[j], sems.at[j])
        for j, source in enumerate((q, f, b, v))
    ] + [
        pltpu.make_async_copy(source, narrow.at[j], sems.at[4 + j])
        for j, source in enumerate((dq, dk, dv))
    ] + [pltpu.make_async_copy(gaps_in, gaps, sems.at[7])]
    for copy in copies:
        copy.start()
    for copy in copies:
        copy.wait()
    half = q.shape[0] // 2
    extra = stacked(
        EXTRA,
        (*thirds(gaps[0:1]), *thirds(gaps[1:2]), *thirds(jnp.full((1, LANES), lam[0], f32))),
    )
    for j in range(4):
        k = j % 3
        folded = jnp.concatenate([narrow[k, :half, :], narrow[k, half:, :]], axis=1)
        block = jnp.concatenate([wide[j], folded, extra], axis=0)
        for c in range(2):
            out[c, j] = block


def norm_kernel(x, gain_in, out, rows, gain, sems):
    copies = (
        pltpu.make_async_copy(x.at[0], rows, sems.at[0]),
        pltpu.make_async_copy(gain_in, gain, sems.at[1]),
    )
    for copy in copies:
        copy.start()
    for copy in copies:
        copy.wait()
    part = rows[...].astype(f32)
    scale = lax.rsqrt(jnp.mean(part * part, axis=-1, keepdims=True) + epsilon)
    done = (part * scale * gain[...]).astype(bf16)
    for k in range(out.shape[0]):
        out[k] = done


def project_kernel(place, rows, weights, out, rhs):
    blocks, packed, _ = weights.shape
    depth = packed * 2 // 3
    half = depth // 2
    wide = weights[:, :depth, :]
    narrow = weights[:, depth:, :].astype(f32)
    first, second = narrow[:, :, :HEAD], narrow[:, :, HEAD:]
    narrow = jnp.concatenate(
        [
            jnp.concatenate([first, first], axis=2),
            jnp.concatenate([second, second], axis=2),
        ],
        axis=1,
    ).astype(bf16)
    rhs[:, :LANES] = wide.reshape(blocks * depth, LANES)
    rhs[:, LANES:] = narrow.reshape(blocks * depth, LANES)
    count, length, width = rows.shape
    whole = dot(rows[...].reshape(count * length, width), rhs[...], ((1,), (0,))).astype(bf16)
    half = length // 2
    lane = lax.broadcasted_iota(jnp.int32, (half, LANES), 1)
    turned = jnp.where(place[0] == 2, HEAD, 0)
    early = lax.rem(lane + turned, LANES) < HEAD
    for k in range(count):
        part = whole[k * length : (k + 1) * length]
        folded = jnp.where(early, part[:half, LANES:], part[half:, LANES:])
        for a in range(2):
            out[a, k, :length] = part[:, :LANES]
            out[a, k, length:] = folded


def swapped(block):
    return jnp.concatenate([block[:, HEAD:], block[:, :HEAD]], axis=1)


def local_kernel(
    place, got, extra_in, gains_in, out, other, query_out, local, read_fwd, read_bwd, gains
):
    extra = extra_in[...].astype(f32)
    gaps = [extra[3 * d : 3 * d + 1] + extra[3 * d + 1 : 3 * d + 2] + extra[3 * d + 2 : 3 * d + 3] for d in range(3)]
    gains[:2] = gains_in[...]
    gains[2:] = gaps[2]
    length = local.shape[0]
    half = length // 2
    odd = place[0] == 1
    mine = place[0] * 4
    row = lax.broadcasted_iota(jnp.int32, (length, length), 0)
    col = lax.broadcasted_iota(jnp.int32, (length, length), 1)
    lane = lax.broadcasted_iota(jnp.int32, (length, LANES), 1)
    lane_head = lax.broadcasted_iota(jnp.int32, (HEAD, LANES), 1)
    masks = row >= col, row <= col
    takens, gones, states, decays = ({}, {}, {}, {})
    for slot in range(2):
        values = got[4 * slot + 3, :length]
        for d in range(2):
            gate = got[4 * slot + 1 + d, :length].astype(f32)
            taken = gaps[d] * jax.nn.sigmoid(-gate)
            kept = jnp.log1p(-taken)
            gone = dot(masks[d].astype(f32), kept, ((1,), (0,)), lax.Precision.HIGHEST)
            total = gone[length - 1 : length] if d == 0 else gone[0:1]
            state = dot(values, (taken * jnp.exp(total - gone)).astype(bf16), ((0,), (0,)))
            takens[slot, d], gones[slot, d] = taken, gone
            states[slot, d] = jnp.where(lane_head < HEAD, state[:HEAD], state[HEAD:])
            decays[slot, d] = jnp.exp(total)
    fwd = decays[1, 0] * states[0, 0] + states[1, 0]
    bwd = decays[0, 1] * states[1, 1] + states[0, 1]
    quarter = HEAD // 2
    part = jnp.concatenate(
        [
            jnp.where(odd, fwd[quarter:], fwd[:quarter]),
            jnp.where(odd, bwd[quarter:], bwd[:quarter]),
        ],
        axis=0,
    )
    out[length : length + HEAD] = part.astype(bf16)
    lines = (*halves(decays[0, 0] * decays[1, 0]), *halves(decays[0, 1] * decays[1, 1]))
    out[length + HEAD :] = stacked(TAIL, lines)
    other[:HEAD] = states[0, 0]
    other[HEAD : 2 * HEAD] = states[1, 1]
    row_tail = lax.broadcasted_iota(jnp.int32, (TAIL, LANES), 0)
    other[2 * HEAD :] = jnp.where(row_tail == 0, decays[0, 0], decays[1, 1])

    keys, worth = got[mine + 1, length:], got[mine + 2, length:]
    lane_half = lane[:half]
    out[:half] = jnp.where(lane_half < HEAD, keys, worth)
    out[half:length] = swapped(jnp.where(lane_half < HEAD, worth, keys))
    folded = got[mine, length:]
    query_out[:half] = folded
    query_out[half:] = swapped(folded)

    queries = got[mine, :length].astype(f32)
    queries = queries * jax.nn.sigmoid(queries)
    values = got[mine + 3, :length]
    weights = [0.0, 0.0]
    for d in range(2):
        gone = jnp.where(odd, gones[1, d], gones[0, d])
        taken = jnp.where(odd, takens[1, d], takens[0, d])
        reader = read_bwd if d else read_fwd
        reader[...] = (queries * jnp.exp(gone)).astype(bf16)
        middle = gone[half : half + 1]
        query_part = queries * jnp.exp(gone - middle)
        key_part = (taken * jnp.exp(middle - gone)).astype(bf16)
        for h in range(2):
            inside = (lane >= h * HEAD) & (lane < (h + 1) * HEAD)
            score = dot(jnp.where(inside, query_part, 0.0).astype(bf16), key_part, ((1,), (1,)))
            weights[h] = weights[h] + jnp.where(masks[d], score, 0.0)
    out_0 = dot(weights[0].astype(bf16), values, ((1,), (0,)))
    out_1 = dot(weights[1].astype(bf16), values, ((1,), (0,)))
    local[...] = jnp.where(lane < HEAD, out_0, out_1)


def stacked(count, lines):
    row = lax.broadcasted_iota(jnp.int32, (count, LANES), 0)
    block = jnp.zeros((count, LANES), f32)
    for k, line in enumerate(lines):
        block = jnp.where(row == k, jnp.broadcast_to(line.astype(f32), (count, LANES)), block)
    return block.astype(bf16)


def halves(value):
    high = value.astype(bf16)
    return high, (value - high.astype(f32)).astype(bf16)


def finish_kernel(
    place, got, other, df_query, local, read_fwd, read_bwd, gains, hg_w, df_w, out, mixed
):
    devices = got.shape[0]
    length = local.shape[0]
    me = place[0]
    lane = lax.broadcasted_iota(jnp.int32, (length, LANES), 1)

    half = HEAD // 2
    pair, odd = me // 2, lax.rem(me, 2) == 1

    def folded(order, passed, k):
        state = jnp.zeros((HEAD, LANES), f32)
        rows = slice(length + k * half, length + (k + 1) * half)
        for w in order:
            fresh = jnp.concatenate([got[2 * w, rows], got[2 * w + 1, rows]], axis=0).astype(f32)
            tail = got[2 * w, length + HEAD :].astype(f32)
            decay = tail[2 * k : 2 * k + 1] + tail[2 * k + 1 : 2 * k + 2]
            state = jnp.where(passed(w), decay * state + fresh, state)
        decay = other[2 * HEAD + k : 2 * HEAD + k + 1]
        joined = decay * state + other[k * HEAD : (k + 1) * HEAD]
        return jnp.where(odd if k == 0 else jnp.logical_not(odd), joined, state).astype(bf16)

    fwd = folded(range(devices // 2), lambda w: w < pair, 0)
    bwd = folded(range(devices // 2 - 1, -1, -1), lambda w: w > pair, 1)
    recurrent = local[...]
    parts = []
    for h in range(2):
        inside = (lane >= h * HEAD) & (lane < (h + 1) * HEAD)
        zero = jnp.zeros((length, LANES), bf16)
        parts.append(
            dot(jnp.where(inside, read_fwd[...], zero), fwd, ((1,), (1,)))
            + dot(jnp.where(inside, read_bwd[...], zero), bwd, ((1,), (1,)))
        )
    recurrent = recurrent + jnp.concatenate(parts, axis=1)
    squares = recurrent * recurrent
    first = jnp.sum(jnp.where(lane < HEAD, squares, 0.0), axis=1, keepdims=True)
    second = jnp.sum(jnp.where(lane < HEAD, 0.0, squares), axis=1, keepdims=True)
    mean = jnp.where(lane < HEAD, first, second) * (1.0 / HEAD)
    mixed[:, :LANES] = (recurrent * lax.rsqrt(mean + epsilon) * gains[0:1]).astype(bf16)

    keys_values = got[:, :length, :].reshape(devices * length, LANES)
    query = df_query[...]
    only = jnp.concatenate(
        [
            jnp.where((lane >= m * DQK) & (lane < (m + 1) * DQK), query, jnp.zeros_like(query))
            for m in range(2)
        ],
        axis=0,
    )
    scores = dot(only, keys_values, ((1,), (1,))) * (DQK ** (-0.5))
    shifted = jnp.exp(scores - jnp.max(scores, axis=-1, keepdims=True))
    totals = jnp.sum(shifted, axis=-1, keepdims=True)
    maps = dot(shifted.astype(bf16), keys_values, ((1,), (0,))) / totals
    weighted = (maps[:length] - gains[2:3] * maps[length:])[:, HEAD:]
    mean = jnp.mean(weighted * weighted, axis=-1, keepdims=True)
    mixed[:, LANES:] = (
        weighted * lax.rsqrt(mean + epsilon) * gains[1:2, :HEAD] * df_factor
    ).astype(bf16)
    out[...] = (
        dot(mixed[:, :LANES], hg_w[...], ((1,), (0,)))
        + dot(mixed[:, LANES:], df_w[...], ((1,), (0,)))
    ).astype(bf16)


def close_kernel(parts, gain, out):
    mixture = parts[0].astype(f32)
    for k in range(1, parts.shape[0]):
        mixture = mixture + parts[k].astype(f32)
    scale = lax.rsqrt(jnp.mean(mixture * mixture, axis=-1, keepdims=True) + epsilon)
    out[0] = (mixture * scale * gain[...]).astype(bf16)


def shards(
    inputs,
    norm_gain,
    hg_query_w,
    hg_fwd_w,
    hg_bwd_w,
    hg_value_w,
    floor_gap,
    hg_norm_gain,
    df_query_w,
    df_key_w,
    df_value_w,
    diff_lambda,
    df_norm_gain,
    out_hg_w,
    out_df_w,
    post_gain,
):
    sp, fs, tp = (lax.axis_size(a) for a in ("sp", "fs", "tp"))
    z, y = lax.axis_index("sp"), lax.axis_index("fs")
    _, length, width = inputs.shape
    depth = hg_query_w.shape[0]
    packed = depth + depth // 2

    vmem = VMEM_SPEC
    normed = pl.pallas_call(
        norm_kernel,
        in_specs=[FAR_SPEC] * 2,
        out_specs=vmem,
        out_shape=pltpu.VMEM((fs, length, width), bf16),
        scratch_shapes=[
            pltpu.VMEM((length, width), bf16),
            pltpu.VMEM((1, width), f32),
            pltpu.SemaphoreType.DMA((2,)),
        ],
        compiler_params=LIMIT,
        name="norm",
    )(there(inputs), there(norm_gain[None]))
    rows = lax.all_to_all(normed, "fs", 0, 0, tiled=True)
    sources = (hg_query_w, hg_fwd_w, hg_bwd_w, hg_value_w, df_query_w, df_key_w, df_value_w)
    sent = pl.pallas_call(
        pack_kernel,
        in_specs=[SMEM_SPEC] + [FAR_SPEC] * 8,
        out_specs=vmem,
        out_shape=pltpu.VMEM((2, fs, packed + EXTRA, LANES), bf16),
        scratch_shapes=[
            pltpu.VMEM((4, depth, LANES), bf16),
            pltpu.VMEM((3, depth, LANES // 2), bf16),
            pltpu.VMEM((2, LANES), f32),
            pltpu.SemaphoreType.DMA((8,)),
        ],
        compiler_params=LIMIT,
        name="pack",
    )(diff_lambda, *map(there, (*sources, floor_gap)))
    share = (lax.axis_index("tp") + z) % 2
    both = lax.all_to_all(
        sent.reshape(2 * fs, packed + EXTRA, LANES),
        ("fs", "tp"),
        0,
        0,
        axis_index_groups=[
            [k * tp + 2 * x + c for c in range(2) for k in range(fs)] for x in range(tp // 2)
        ],
        tiled=True,
    )
    mine = lax.dynamic_slice_in_dim(both, share * fs, fs, 0)
    extra = mine[0, packed:]
    rings = [[k * tp + (t ^ (k % 2)) for k in range(sp)] for t in range(tp)]
    weights = lax.all_gather(
        mine[None, :, :packed], ("sp", "tp"), axis=0, tiled=True, axis_index_groups=rings
    )
    weights = weights.reshape(sp * fs, packed, LANES)
    projected = pl.pallas_call(
        project_kernel,
        in_specs=[SMEM_SPEC] + [vmem] * 2,
        out_specs=vmem,
        out_shape=pltpu.VMEM((2, fs, length + length // 2, LANES), bf16),
        scratch_shapes=[pltpu.VMEM((width, 2 * LANES), bf16)],
        compiler_params=LIMIT,
        name="project",
    )(y.astype(jnp.int32)[None], here(rows), here(weights))
    groups = [
        [((2 * i + a) * fs + k) * tp + (t ^ a) for a in range(2) for k in range(fs)]
        for i in range(sp // 2)
        for t in range(tp)
    ]
    got = lax.all_to_all(
        projected.reshape(2 * fs, length + length // 2, LANES),
        ("sp", "fs", "tp"),
        0,
        0,
        axis_index_groups=groups,
        tiled=True,
    )
    swap = [(k * tp + t, k * tp + (t ^ (k % 2))) for k in range(sp) for t in range(tp)]
    hg_rows = lax.ppermute(out_hg_w, ("sp", "tp"), swap)
    df_rows = lax.ppermute(out_df_w, ("sp", "tp"), swap)

    place = z.astype(jnp.int32)[None]
    gains = jnp.concatenate([hg_norm_gain, hg_norm_gain, df_norm_gain, df_norm_gain])
    joined, other, query, local, read_fwd, read_bwd, gains = pl.pallas_call(
        local_kernel,
        in_specs=[SMEM_SPEC] + [vmem] * 3,
        out_specs=[vmem] * 7,
        out_shape=[
            pltpu.VMEM((length + HEAD + TAIL, LANES), bf16),
            pltpu.VMEM((2 * HEAD + TAIL, LANES), f32),
            pltpu.VMEM((length, LANES), bf16),
            pltpu.VMEM((length, LANES), f32),
            pltpu.VMEM((length, LANES), bf16),
            pltpu.VMEM((length, LANES), bf16),
            pltpu.VMEM((3, LANES), f32),
        ],
        compiler_params=LIMIT,
        name="local",
    )(place % 2, here(got), here(extra), here(gains.reshape(2, LANES)))
    arrived = lax.all_gather(
        joined[None], ("sp", "tp"), axis=0, tiled=True, axis_index_groups=rings
    )
    partial = pl.pallas_call(
        finish_kernel,
        in_specs=[SMEM_SPEC] + [vmem] * 9,
        out_specs=vmem,
        out_shape=pltpu.VMEM((length, width), bf16),
        scratch_shapes=[pltpu.VMEM((length, LANES + HEAD), bf16)],
        compiler_params=LIMIT,
        name="finish",
    )(
        place,
        here(arrived),
        here(other),
        here(query),
        here(local),
        here(read_fwd),
        here(read_bwd),
        here(gains),
        here(hg_rows),
        here(df_rows),
    )
    parts = lax.all_to_all(
        partial.reshape(tp, length // tp, width), "tp", 0, 0, tiled=True
    )
    return pl.pallas_call(
        close_kernel,
        out_shape=jax.ShapeDtypeStruct((1, length // tp, width), bf16),
        compiler_params=LIMIT,
        name="close",
    )(here(parts), post_gain[None])


def solution(mesh):
    rows = P(("sp", "fs"), "tp")
    in_specs = (
        P("fs", "sp", None),
        P(),
        rows,
        rows,
        rows,
        rows,
        P(None, "tp"),
        P(),
        rows,
        rows,
        rows,
        P("tp"),
        P(),
        P("tp", None),
        P("tp", None),
        P(),
    )
    out_specs = P("fs", ("sp", "tp"), None)
    return jax.shard_map(shards, mesh=mesh, in_specs=in_specs, out_specs=out_specs, check_vma=False)
```

```python
import jax
import jax.numpy as jnp
from jax import lax
from jax.experimental import pallas as pl
from jax.experimental.pallas import tpu as pltpu
from jax.sharding import PartitionSpec as P

HEAD = 64
DQK = 32
LANES = 128
TAIL = 8
EXTRA = 16

epsilon = 1e-06
df_factor = 0.8
f32 = jnp.float32
bf16 = jnp.bfloat16

SMEM_SPEC = pl.BlockSpec(memory_space=pltpu.SMEM)
VMEM_SPEC = pl.BlockSpec(memory_space=pltpu.VMEM)
LIMIT = pltpu.CompilerParams(vmem_limit_bytes=24 * 2**20)


FAR_SPEC = pl.BlockSpec(memory_space=pltpu.HBM)


def there(array):
    return pltpu.with_memory_space_constraint(array, pltpu.HBM)


def here(array):
    return pltpu.with_memory_space_constraint(array, pltpu.VMEM)


def dot(a, b, dims, precision=None):
    return lax.dot_general(a, b, (dims, ((), ())), precision=precision, preferred_element_type=f32)


def thirds(value):
    pieces = []
    for _ in range(3):
        pieces.append(value.astype(bf16))
        value = value - pieces[-1].astype(f32)
    return pieces


def pack_kernel(q, f, b, v, dq, dk, dv, gaps_in, out, wide, narrow, gaps, sems):
    copies = [
        pltpu.make_async_copy(source, wide.at[j], sems.at[j])
        for j, source in enumerate((q, f, b, v))
    ] + [
        pltpu.make_async_copy(source, narrow.at[j], sems.at[4 + j])
        for j, source in enumerate((dq, dk, dv))
    ] + [pltpu.make_async_copy(gaps_in, gaps, sems.at[7])]
    for copy in copies:
        copy.start()
    for copy in copies:
        copy.wait()
    half = q.shape[0] // 2
    extra = stacked(EXTRA, (*thirds(gaps[0:1]), *thirds(gaps[1:2])))
    for j in range(4):
        k = j % 3
        folded = jnp.concatenate([narrow[k, :half, :], narrow[k, half:, :]], axis=1)
        block = jnp.concatenate([wide[j], folded, extra], axis=0)
        for c in range(2):
            out[c, j] = block


def norm_kernel(x, gain_in, out, rows, gain, sems):
    copies = (
        pltpu.make_async_copy(x.at[0], rows, sems.at[0]),
        pltpu.make_async_copy(gain_in, gain, sems.at[1]),
    )
    for copy in copies:
        copy.start()
    for copy in copies:
        copy.wait()
    part = rows[...].astype(f32)
    scale = lax.rsqrt(jnp.mean(part * part, axis=-1, keepdims=True) + epsilon)
    done = (part * scale * gain[...]).astype(bf16)
    for k in range(out.shape[0]):
        out[k] = done


def project_kernel(place, rows, weights, out, rhs):
    blocks, packed, _ = weights.shape
    depth = packed * 2 // 3
    half = depth // 2
    wide = weights[:, :depth, :]
    narrow = weights[:, depth:, :].astype(f32)
    first, second = narrow[:, :, :HEAD], narrow[:, :, HEAD:]
    narrow = jnp.concatenate(
        [
            jnp.concatenate([first, first], axis=2),
            jnp.concatenate([second, second], axis=2),
        ],
        axis=1,
    ).astype(bf16)
    rhs[:, :LANES] = wide.reshape(blocks * depth, LANES)
    rhs[:, LANES:] = narrow.reshape(blocks * depth, LANES)
    count, length, width = rows.shape
    whole = dot(rows[...].reshape(count * length, width), rhs[...], ((1,), (0,))).astype(bf16)
    half = length // 2
    lane = lax.broadcasted_iota(jnp.int32, (half, LANES), 1)
    turned = jnp.where(place[0] == 2, HEAD, 0)
    early = lax.rem(lane + turned, LANES) < HEAD
    for k in range(count):
        part = whole[k * length : (k + 1) * length]
        folded = jnp.where(early, part[:half, LANES:], part[half:, LANES:])
        for a in range(2):
            out[a, k, :length] = part[:, :LANES]
            out[a, k, length:] = folded


def swapped(block):
    return jnp.concatenate([block[:, HEAD:], block[:, :HEAD]], axis=1)


def local_kernel(
    place, lam, got, extra_in, gains_in, out, other, query_out, local, read_fwd, read_bwd, gains
):
    extra = extra_in[...].astype(f32)
    gaps = [extra[3 * d : 3 * d + 1] + extra[3 * d + 1 : 3 * d + 2] + extra[3 * d + 2 : 3 * d + 3] for d in range(2)]
    gains[...] = gains_in[...]
    length = local.shape[0]
    half = length // 2
    odd = place[0] == 1
    mine = place[0] * 4
    row = lax.broadcasted_iota(jnp.int32, (length, length), 0)
    col = lax.broadcasted_iota(jnp.int32, (length, length), 1)
    lane = lax.broadcasted_iota(jnp.int32, (length, LANES), 1)
    lane_head = lax.broadcasted_iota(jnp.int32, (HEAD, LANES), 1)
    masks = row >= col, row <= col
    takens, gones, states, decays = ({}, {}, {}, {})
    for slot in range(2):
        values = got[4 * slot + 3, :length]
        for d in range(2):
            gate = got[4 * slot + 1 + d, :length].astype(f32)
            taken = gaps[d] * jax.nn.sigmoid(-gate)
            kept = jnp.log1p(-taken)
            gone = dot(masks[d].astype(f32), kept, ((1,), (0,)), lax.Precision.HIGHEST)
            total = gone[length - 1 : length] if d == 0 else gone[0:1]
            state = dot(values, (taken * jnp.exp(total - gone)).astype(bf16), ((0,), (0,)))
            takens[slot, d], gones[slot, d] = taken, gone
            states[slot, d] = jnp.where(lane_head < HEAD, state[:HEAD], state[HEAD:])
            decays[slot, d] = jnp.exp(total)
    fwd = decays[1, 0] * states[0, 0] + states[1, 0]
    bwd = decays[0, 1] * states[1, 1] + states[0, 1]
    quarter = HEAD // 2
    part = jnp.concatenate(
        [
            jnp.where(odd, fwd[quarter:], fwd[:quarter]),
            jnp.where(odd, bwd[quarter:], bwd[:quarter]),
        ],
        axis=0,
    )
    out[length : length + HEAD] = part.astype(bf16)
    lines = (*halves(decays[0, 0] * decays[1, 0]), *halves(decays[0, 1] * decays[1, 1]))
    lines = (*lines, *thirds(jnp.full((1, LANES), lam[0], f32)))
    out[length + HEAD :] = stacked(TAIL, lines)
    other[:HEAD] = states[0, 0]
    other[HEAD : 2 * HEAD] = states[1, 1]
    row_tail = lax.broadcasted_iota(jnp.int32, (TAIL, LANES), 0)
    other[2 * HEAD :] = jnp.where(row_tail == 0, decays[0, 0], decays[1, 1])

    keys, worth = got[mine + 1, length:], got[mine + 2, length:]
    lane_half = lane[:half]
    out[:half] = jnp.where(lane_half < HEAD, keys, worth)
    out[half:length] = swapped(jnp.where(lane_half < HEAD, worth, keys))
    folded = got[mine, length:]
    query_out[:half] = folded
    query_out[half:] = swapped(folded)

    queries = got[mine, :length].astype(f32)
    queries = queries * jax.nn.sigmoid(queries)
    values = got[mine + 3, :length]
    weights = [0.0, 0.0]
    for d in range(2):
        gone = jnp.where(odd, gones[1, d], gones[0, d])
        taken = jnp.where(odd, takens[1, d], takens[0, d])
        reader = read_bwd if d else read_fwd
        reader[...] = (queries * jnp.exp(gone)).astype(bf16)
        middle = gone[half : half + 1]
        query_part = queries * jnp.exp(gone - middle)
        key_part = (taken * jnp.exp(middle - gone)).astype(bf16)
        for h in range(2):
            inside = (lane >= h * HEAD) & (lane < (h + 1) * HEAD)
            score = dot(jnp.where(inside, query_part, 0.0).astype(bf16), key_part, ((1,), (1,)))
            weights[h] = weights[h] + jnp.where(masks[d], score, 0.0)
    out_0 = dot(weights[0].astype(bf16), values, ((1,), (0,)))
    out_1 = dot(weights[1].astype(bf16), values, ((1,), (0,)))
    local[...] = jnp.where(lane < HEAD, out_0, out_1)


def stacked(count, lines):
    row = lax.broadcasted_iota(jnp.int32, (count, LANES), 0)
    block = jnp.zeros((count, LANES), f32)
    for k, line in enumerate(lines):
        block = jnp.where(row == k, jnp.broadcast_to(line.astype(f32), (count, LANES)), block)
    return block.astype(bf16)


def halves(value):
    high = value.astype(bf16)
    return high, (value - high.astype(f32)).astype(bf16)


def finish_kernel(
    place, got, other, df_query, local, read_fwd, read_bwd, gains, hg_w, df_w, out, mixed
):
    devices = got.shape[0]
    length = local.shape[0]
    me = place[0]
    lane = lax.broadcasted_iota(jnp.int32, (length, LANES), 1)

    half = HEAD // 2
    pair, odd = me // 2, lax.rem(me, 2) == 1

    def folded(order, passed, k):
        state = jnp.zeros((HEAD, LANES), f32)
        rows = slice(length + k * half, length + (k + 1) * half)
        for w in order:
            fresh = jnp.concatenate([got[2 * w, rows], got[2 * w + 1, rows]], axis=0).astype(f32)
            tail = got[2 * w, length + HEAD :].astype(f32)
            decay = tail[2 * k : 2 * k + 1] + tail[2 * k + 1 : 2 * k + 2]
            state = jnp.where(passed(w), decay * state + fresh, state)
        decay = other[2 * HEAD + k : 2 * HEAD + k + 1]
        joined = decay * state + other[k * HEAD : (k + 1) * HEAD]
        return jnp.where(odd if k == 0 else jnp.logical_not(odd), joined, state).astype(bf16)

    fwd = folded(range(devices // 2), lambda w: w < pair, 0)
    bwd = folded(range(devices // 2 - 1, -1, -1), lambda w: w > pair, 1)
    recurrent = local[...]
    parts = []
    for h in range(2):
        inside = (lane >= h * HEAD) & (lane < (h + 1) * HEAD)
        zero = jnp.zeros((length, LANES), bf16)
        parts.append(
            dot(jnp.where(inside, read_fwd[...], zero), fwd, ((1,), (1,)))
            + dot(jnp.where(inside, read_bwd[...], zero), bwd, ((1,), (1,)))
        )
    recurrent = recurrent + jnp.concatenate(parts, axis=1)
    squares = recurrent * recurrent
    first = jnp.sum(jnp.where(lane < HEAD, squares, 0.0), axis=1, keepdims=True)
    second = jnp.sum(jnp.where(lane < HEAD, 0.0, squares), axis=1, keepdims=True)
    mean = jnp.where(lane < HEAD, first, second) * (1.0 / HEAD)
    mixed[:, :LANES] = (recurrent * lax.rsqrt(mean + epsilon) * gains[0:1]).astype(bf16)

    keys_values = got[:, :length, :].reshape(devices * length, LANES)
    query = df_query[...]
    only = jnp.concatenate(
        [
            jnp.where((lane >= m * DQK) & (lane < (m + 1) * DQK), query, jnp.zeros_like(query))
            for m in range(2)
        ],
        axis=0,
    )
    scores = dot(only, keys_values, ((1,), (1,))) * (DQK ** (-0.5))
    shifted = jnp.exp(scores - jnp.max(scores, axis=-1, keepdims=True))
    totals = jnp.sum(shifted, axis=-1, keepdims=True)
    maps = dot(shifted.astype(bf16), keys_values, ((1,), (0,))) / totals
    first = got[0, length + HEAD :].astype(f32)
    lam = first[4:5] + first[5:6] + first[6:7]
    weighted = (maps[:length] - lam * maps[length:])[:, HEAD:]
    mean = jnp.mean(weighted * weighted, axis=-1, keepdims=True)
    mixed[:, LANES:] = (
        weighted * lax.rsqrt(mean + epsilon) * gains[1:2, :HEAD] * df_factor
    ).astype(bf16)
    out[...] = (
        dot(mixed[:, :LANES], hg_w[...], ((1,), (0,)))
        + dot(mixed[:, LANES:], df_w[...], ((1,), (0,)))
    ).astype(bf16)


def close_kernel(parts, gain, out):
    mixture = parts[0].astype(f32)
    for k in range(1, parts.shape[0]):
        mixture = mixture + parts[k].astype(f32)
    scale = lax.rsqrt(jnp.mean(mixture * mixture, axis=-1, keepdims=True) + epsilon)
    out[0] = (mixture * scale * gain[...]).astype(bf16)


def shards(
    inputs,
    norm_gain,
    hg_query_w,
    hg_fwd_w,
    hg_bwd_w,
    hg_value_w,
    floor_gap,
    hg_norm_gain,
    df_query_w,
    df_key_w,
    df_value_w,
    diff_lambda,
    df_norm_gain,
    out_hg_w,
    out_df_w,
    post_gain,
):
    sp, fs, tp = (lax.axis_size(a) for a in ("sp", "fs", "tp"))
    z, y = lax.axis_index("sp"), lax.axis_index("fs")
    _, length, width = inputs.shape
    depth = hg_query_w.shape[0]
    packed = depth + depth // 2

    vmem = VMEM_SPEC
    normed = pl.pallas_call(
        norm_kernel,
        in_specs=[FAR_SPEC] * 2,
        out_specs=vmem,
        out_shape=pltpu.VMEM((fs, length, width), bf16),
        scratch_shapes=[
            pltpu.VMEM((length, width), bf16),
            pltpu.VMEM((1, width), f32),
            pltpu.SemaphoreType.DMA((2,)),
        ],
        compiler_params=LIMIT,
        name="norm",
    )(there(inputs), there(norm_gain[None]))
    rows = lax.all_to_all(normed, "fs", 0, 0, tiled=True)
    sources = (hg_query_w, hg_fwd_w, hg_bwd_w, hg_value_w, df_query_w, df_key_w, df_value_w)
    sent = pl.pallas_call(
        pack_kernel,
        in_specs=[FAR_SPEC] * 8,
        out_specs=vmem,
        out_shape=pltpu.VMEM((2, fs, packed + EXTRA, LANES), bf16),
        scratch_shapes=[
            pltpu.VMEM((4, depth, LANES), bf16),
            pltpu.VMEM((3, depth, LANES // 2), bf16),
            pltpu.VMEM((2, LANES), f32),
            pltpu.SemaphoreType.DMA((8,)),
        ],
        compiler_params=LIMIT,
        name="pack",
    )(*map(there, (*sources, floor_gap)))
    share = (lax.axis_index("tp") + z // 2) % 2
    both = lax.all_to_all(
        sent.reshape(2 * fs, packed + EXTRA, LANES),
        ("fs", "tp"),
        0,
        0,
        axis_index_groups=[
            [k * tp + 2 * x + c for c in range(2) for k in range(fs)] for x in range(tp // 2)
        ],
        tiled=True,
    )
    mine = lax.dynamic_slice_in_dim(both, share * fs, fs, 0)
    extra = mine[0, packed:]
    rings = [[k * tp + (t ^ (k // 2 % 2)) for k in range(sp)] for t in range(tp)]
    weights = lax.all_gather(
        mine[None, :, :packed], ("sp", "tp"), axis=0, tiled=True, axis_index_groups=rings
    )
    weights = weights.reshape(sp * fs, packed, LANES)
    projected = pl.pallas_call(
        project_kernel,
        in_specs=[SMEM_SPEC] + [vmem] * 2,
        out_specs=vmem,
        out_shape=pltpu.VMEM((2, fs, length + length // 2, LANES), bf16),
        scratch_shapes=[pltpu.VMEM((width, 2 * LANES), bf16)],
        compiler_params=LIMIT,
        name="project",
    )(y.astype(jnp.int32)[None], here(rows), here(weights))
    groups = [
        [((2 * i + a) * fs + k) * tp + t for a in range(2) for k in range(fs)]
        for i in range(sp // 2)
        for t in range(tp)
    ]
    got = lax.all_to_all(
        projected.reshape(2 * fs, length + length // 2, LANES),
        ("sp", "fs", "tp"),
        0,
        0,
        axis_index_groups=groups,
        tiled=True,
    )
    swap = [(k * tp + t, k * tp + (t ^ (k // 2 % 2))) for k in range(sp) for t in range(tp)]
    hg_rows = lax.ppermute(out_hg_w, ("sp", "tp"), swap)
    df_rows = lax.ppermute(out_df_w, ("sp", "tp"), swap)

    place = z.astype(jnp.int32)[None]
    gains = jnp.concatenate([hg_norm_gain, hg_norm_gain, df_norm_gain, df_norm_gain])
    joined, other, query, local, read_fwd, read_bwd, gains = pl.pallas_call(
        local_kernel,
        in_specs=[SMEM_SPEC] * 2 + [vmem] * 3,
        out_specs=[vmem] * 7,
        out_shape=[
            pltpu.VMEM((length + HEAD + TAIL, LANES), bf16),
            pltpu.VMEM((2 * HEAD + TAIL, LANES), f32),
            pltpu.VMEM((length, LANES), bf16),
            pltpu.VMEM((length, LANES), f32),
            pltpu.VMEM((length, LANES), bf16),
            pltpu.VMEM((length, LANES), bf16),
            pltpu.VMEM((2, LANES), f32),
        ],
        compiler_params=LIMIT,
        name="local",
    )(place % 2, diff_lambda, here(got), here(extra), here(gains.reshape(2, LANES)))
    arrived = lax.all_gather(
        joined[None], ("sp", "tp"), axis=0, tiled=True, axis_index_groups=rings
    )
    partial = pl.pallas_call(
        finish_kernel,
        in_specs=[SMEM_SPEC] + [vmem] * 9,
        out_specs=vmem,
        out_shape=pltpu.VMEM((length, width), bf16),
        scratch_shapes=[pltpu.VMEM((length, LANES + HEAD), bf16)],
        compiler_params=LIMIT,
        name="finish",
    )(
        place,
        here(arrived),
        here(other),
        here(query),
        here(local),
        here(read_fwd),
        here(read_bwd),
        here(gains),
        here(hg_rows),
        here(df_rows),
    )
    parts = lax.all_to_all(
        partial.reshape(tp, length // tp, width), "tp", 0, 0, tiled=True
    )
    return pl.pallas_call(
        close_kernel,
        out_shape=jax.ShapeDtypeStruct((1, length // tp, width), bf16),
        compiler_params=LIMIT,
        name="close",
    )(here(parts), post_gain[None])


def solution(mesh):
    rows = P(("sp", "fs"), "tp")
    in_specs = (
        P("fs", "sp", None),
        P(),
        rows,
        rows,
        rows,
        rows,
        P(None, "tp"),
        P(),
        rows,
        rows,
        rows,
        P("tp"),
        P(),
        P("tp", None),
        P("tp", None),
        P(),
    )
    out_specs = P("fs", ("sp", "tp"), None)
    return jax.shard_map(shards, mesh=mesh, in_specs=in_specs, out_specs=out_specs, check_vma=False)
```

```python
import jax
import jax.numpy as jnp
from jax import lax
from jax.experimental import pallas as pl
from jax.experimental.pallas import tpu as pltpu
from jax.sharding import PartitionSpec as P

HEAD = 64
DQK = 32
LANES = 128
TAIL = 8
EXTRA = 16

epsilon = 1e-06
df_factor = 0.8
f32 = jnp.float32
bf16 = jnp.bfloat16

SMEM_SPEC = pl.BlockSpec(memory_space=pltpu.SMEM)
VMEM_SPEC = pl.BlockSpec(memory_space=pltpu.VMEM)
LIMIT = pltpu.CompilerParams(vmem_limit_bytes=24 * 2**20)


FAR_SPEC = pl.BlockSpec(memory_space=pltpu.HBM)


def there(array):
    return pltpu.with_memory_space_constraint(array, pltpu.HBM)


def here(array):
    return pltpu.with_memory_space_constraint(array, pltpu.VMEM)


def dot(a, b, dims, precision=None):
    return lax.dot_general(a, b, (dims, ((), ())), precision=precision, preferred_element_type=f32)


def thirds(value):
    pieces = []
    for _ in range(3):
        pieces.append(value.astype(bf16))
        value = value - pieces[-1].astype(f32)
    return pieces


def pack_kernel(q, f, b, v, dq, dk, dv, gaps_in, out, wide, narrow, gaps, sems):
    copies = [
        pltpu.make_async_copy(source, wide.at[j], sems.at[j])
        for j, source in enumerate((q, f, b, v))
    ] + [
        pltpu.make_async_copy(source, narrow.at[j], sems.at[4 + j])
        for j, source in enumerate((dq, dk, dv))
    ] + [pltpu.make_async_copy(gaps_in, gaps, sems.at[7])]
    for copy in copies:
        copy.start()
    for copy in copies:
        copy.wait()
    half = q.shape[0] // 2
    extra = stacked(EXTRA, (*thirds(gaps[0:1]), *thirds(gaps[1:2])))
    for j in range(4):
        k = j % 3
        folded = jnp.concatenate([narrow[k, :half, :], narrow[k, half:, :]], axis=1)
        block = jnp.concatenate([wide[j], folded, extra], axis=0)
        for c in range(2):
            out[c, j] = block


def norm_kernel(x, gain_in, hg_w, df_w, out, outer, rows, gain, joined, sems):
    copies = (
        pltpu.make_async_copy(x.at[0], rows, sems.at[0]),
        pltpu.make_async_copy(gain_in, gain, sems.at[1]),
    )
    late = (
        pltpu.make_async_copy(hg_w, joined.at[:LANES], sems.at[2]),
        pltpu.make_async_copy(df_w, joined.at[LANES:], sems.at[3]),
    )
    for copy in (*copies, *late):
        copy.start()
    for copy in (*copies, *late):
        copy.wait()
    store = pltpu.make_async_copy(joined, outer, sems.at[4])
    store.start()
    part = rows[...].astype(f32)
    scale = lax.rsqrt(jnp.mean(part * part, axis=-1, keepdims=True) + epsilon)
    done = (part * scale * gain[...]).astype(bf16)
    for k in range(out.shape[0]):
        out[k] = done
    store.wait()


def project_kernel(place, rows, weights, out, rhs):
    blocks, packed, _ = weights.shape
    depth = packed * 2 // 3
    half = depth // 2
    wide = weights[:, :depth, :]
    narrow = weights[:, depth:, :].astype(f32)
    first, second = narrow[:, :, :HEAD], narrow[:, :, HEAD:]
    narrow = jnp.concatenate(
        [
            jnp.concatenate([first, first], axis=2),
            jnp.concatenate([second, second], axis=2),
        ],
        axis=1,
    ).astype(bf16)
    rhs[:, :LANES] = wide.reshape(blocks * depth, LANES)
    rhs[:, LANES:] = narrow.reshape(blocks * depth, LANES)
    count, length, width = rows.shape
    whole = dot(rows[...].reshape(count * length, width), rhs[...], ((1,), (0,))).astype(bf16)
    half = length // 2
    lane = lax.broadcasted_iota(jnp.int32, (half, LANES), 1)
    turned = jnp.where(place[0] == 2, HEAD, 0)
    early = lax.rem(lane + turned, LANES) < HEAD
    for k in range(count):
        part = whole[k * length : (k + 1) * length]
        folded = jnp.where(early, part[:half, LANES:], part[half:, LANES:])
        for a in range(2):
            out[a, k, :length] = part[:, :LANES]
            out[a, k, length:] = folded


def swapped(block):
    return jnp.concatenate([block[:, HEAD:], block[:, :HEAD]], axis=1)


def local_kernel(
    place, lam, got, extra_in, gains_in, out, other, query_out, local, read_fwd, read_bwd, gains
):
    extra = extra_in[...].astype(f32)
    gaps = [extra[3 * d : 3 * d + 1] + extra[3 * d + 1 : 3 * d + 2] + extra[3 * d + 2 : 3 * d + 3] for d in range(2)]
    gains[...] = gains_in[...]
    length = local.shape[0]
    half = length // 2
    odd = place[0] == 1
    mine = place[0] * 4
    row = lax.broadcasted_iota(jnp.int32, (length, length), 0)
    col = lax.broadcasted_iota(jnp.int32, (length, length), 1)
    lane = lax.broadcasted_iota(jnp.int32, (length, LANES), 1)
    lane_head = lax.broadcasted_iota(jnp.int32, (HEAD, LANES), 1)
    masks = row >= col, row <= col
    takens, gones, states, decays = ({}, {}, {}, {})
    for slot in range(2):
        values = got[4 * slot + 3, :length]
        for d in range(2):
            gate = got[4 * slot + 1 + d, :length].astype(f32)
            taken = gaps[d] * jax.nn.sigmoid(-gate)
            kept = jnp.log1p(-taken)
            gone = dot(masks[d].astype(f32), kept, ((1,), (0,)), lax.Precision.HIGHEST)
            total = gone[length - 1 : length] if d == 0 else gone[0:1]
            state = dot(values, (taken * jnp.exp(total - gone)).astype(bf16), ((0,), (0,)))
            takens[slot, d], gones[slot, d] = taken, gone
            states[slot, d] = jnp.where(lane_head < HEAD, state[:HEAD], state[HEAD:])
            decays[slot, d] = jnp.exp(total)
    fwd = decays[1, 0] * states[0, 0] + states[1, 0]
    bwd = decays[0, 1] * states[1, 1] + states[0, 1]
    quarter = HEAD // 2
    part = jnp.concatenate(
        [
            jnp.where(odd, fwd[quarter:], fwd[:quarter]),
            jnp.where(odd, bwd[quarter:], bwd[:quarter]),
        ],
        axis=0,
    )
    out[length : length + HEAD] = part.astype(bf16)
    lines = (*halves(decays[0, 0] * decays[1, 0]), *halves(decays[0, 1] * decays[1, 1]))
    lines = (*lines, *thirds(jnp.full((1, LANES), lam[0], f32)))
    out[length + HEAD :] = stacked(TAIL, lines)
    other[:HEAD] = states[0, 0]
    other[HEAD : 2 * HEAD] = states[1, 1]
    row_tail = lax.broadcasted_iota(jnp.int32, (TAIL, LANES), 0)
    other[2 * HEAD :] = jnp.where(row_tail == 0, decays[0, 0], decays[1, 1])

    keys, worth = got[mine + 1, length:], got[mine + 2, length:]
    lane_half = lane[:half]
    out[:half] = jnp.where(lane_half < HEAD, keys, worth)
    out[half:length] = swapped(jnp.where(lane_half < HEAD, worth, keys))
    folded = got[mine, length:]
    query_out[:half] = folded
    query_out[half:] = swapped(folded)

    queries = got[mine, :length].astype(f32)
    queries = queries * jax.nn.sigmoid(queries)
    values = got[mine + 3, :length]
    weights = [0.0, 0.0]
    for d in range(2):
        gone = jnp.where(odd, gones[1, d], gones[0, d])
        taken = jnp.where(odd, takens[1, d], takens[0, d])
        reader = read_bwd if d else read_fwd
        reader[...] = (queries * jnp.exp(gone)).astype(bf16)
        middle = gone[half : half + 1]
        query_part = queries * jnp.exp(gone - middle)
        key_part = (taken * jnp.exp(middle - gone)).astype(bf16)
        for h in range(2):
            inside = (lane >= h * HEAD) & (lane < (h + 1) * HEAD)
            score = dot(jnp.where(inside, query_part, 0.0).astype(bf16), key_part, ((1,), (1,)))
            weights[h] = weights[h] + jnp.where(masks[d], score, 0.0)
    out_0 = dot(weights[0].astype(bf16), values, ((1,), (0,)))
    out_1 = dot(weights[1].astype(bf16), values, ((1,), (0,)))
    local[...] = jnp.where(lane < HEAD, out_0, out_1)


def stacked(count, lines):
    row = lax.broadcasted_iota(jnp.int32, (count, LANES), 0)
    block = jnp.zeros((count, LANES), f32)
    for k, line in enumerate(lines):
        block = jnp.where(row == k, jnp.broadcast_to(line.astype(f32), (count, LANES)), block)
    return block.astype(bf16)


def halves(value):
    high = value.astype(bf16)
    return high, (value - high.astype(f32)).astype(bf16)


def finish_kernel(
    place, got, other, df_query, local, read_fwd, read_bwd, gains, outer, out, mixed
):
    devices = got.shape[0]
    length = local.shape[0]
    me = place[0]
    lane = lax.broadcasted_iota(jnp.int32, (length, LANES), 1)

    half = HEAD // 2
    pair, odd = me // 2, lax.rem(me, 2) == 1

    def folded(order, passed, k):
        state = jnp.zeros((HEAD, LANES), f32)
        rows = slice(length + k * half, length + (k + 1) * half)
        for w in order:
            fresh = jnp.concatenate([got[2 * w, rows], got[2 * w + 1, rows]], axis=0).astype(f32)
            tail = got[2 * w, length + HEAD :].astype(f32)
            decay = tail[2 * k : 2 * k + 1] + tail[2 * k + 1 : 2 * k + 2]
            state = jnp.where(passed(w), decay * state + fresh, state)
        decay = other[2 * HEAD + k : 2 * HEAD + k + 1]
        joined = decay * state + other[k * HEAD : (k + 1) * HEAD]
        return jnp.where(odd if k == 0 else jnp.logical_not(odd), joined, state).astype(bf16)

    fwd = folded(range(devices // 2), lambda w: w < pair, 0)
    bwd = folded(range(devices // 2 - 1, -1, -1), lambda w: w > pair, 1)
    recurrent = local[...]
    parts = []
    for h in range(2):
        inside = (lane >= h * HEAD) & (lane < (h + 1) * HEAD)
        zero = jnp.zeros((length, LANES), bf16)
        parts.append(
            dot(jnp.where(inside, read_fwd[...], zero), fwd, ((1,), (1,)))
            + dot(jnp.where(inside, read_bwd[...], zero), bwd, ((1,), (1,)))
        )
    recurrent = recurrent + jnp.concatenate(parts, axis=1)
    squares = recurrent * recurrent
    first = jnp.sum(jnp.where(lane < HEAD, squares, 0.0), axis=1, keepdims=True)
    second = jnp.sum(jnp.where(lane < HEAD, 0.0, squares), axis=1, keepdims=True)
    mean = jnp.where(lane < HEAD, first, second) * (1.0 / HEAD)
    mixed[:, :LANES] = (recurrent * lax.rsqrt(mean + epsilon) * gains[0:1]).astype(bf16)

    keys_values = got[:, :length, :].reshape(devices * length, LANES)
    query = df_query[...]
    only = jnp.concatenate(
        [
            jnp.where((lane >= m * DQK) & (lane < (m + 1) * DQK), query, jnp.zeros_like(query))
            for m in range(2)
        ],
        axis=0,
    )
    scores = dot(only, keys_values, ((1,), (1,))) * (DQK ** (-0.5))
    shifted = jnp.exp(scores - jnp.max(scores, axis=-1, keepdims=True))
    totals = jnp.sum(shifted, axis=-1, keepdims=True)
    maps = dot(shifted.astype(bf16), keys_values, ((1,), (0,))) / totals
    first = got[0, length + HEAD :].astype(f32)
    lam = first[4:5] + first[5:6] + first[6:7]
    weighted = (maps[:length] - lam * maps[length:])[:, HEAD:]
    mean = jnp.mean(weighted * weighted, axis=-1, keepdims=True)
    mixed[:, LANES:] = (
        weighted * lax.rsqrt(mean + epsilon) * gains[1:2, :HEAD] * df_factor
    ).astype(bf16)
    out[...] = dot(mixed[...], outer[...], ((1,), (0,))).astype(bf16)


def close_kernel(parts, gain, out):
    mixture = parts[0].astype(f32)
    for k in range(1, parts.shape[0]):
        mixture = mixture + parts[k].astype(f32)
    scale = lax.rsqrt(jnp.mean(mixture * mixture, axis=-1, keepdims=True) + epsilon)
    out[0] = (mixture * scale * gain[...]).astype(bf16)


def shards(
    inputs,
    norm_gain,
    hg_query_w,
    hg_fwd_w,
    hg_bwd_w,
    hg_value_w,
    floor_gap,
    hg_norm_gain,
    df_query_w,
    df_key_w,
    df_value_w,
    diff_lambda,
    df_norm_gain,
    out_hg_w,
    out_df_w,
    post_gain,
):
    sp, fs, tp = (lax.axis_size(a) for a in ("sp", "fs", "tp"))
    z, y = lax.axis_index("sp"), lax.axis_index("fs")
    _, length, width = inputs.shape
    depth = hg_query_w.shape[0]
    packed = depth + depth // 2

    vmem = VMEM_SPEC
    normed, outer = pl.pallas_call(
        norm_kernel,
        in_specs=[FAR_SPEC] * 4,
        out_specs=[pl.BlockSpec((fs, length, width), lambda: (0, 0, 0)), FAR_SPEC],
        out_shape=[
            pltpu.HBM((fs, length, width), bf16),
            pltpu.HBM((LANES + HEAD, width), bf16),
        ],
        scratch_shapes=[
            pltpu.VMEM((length, width), bf16),
            pltpu.VMEM((1, width), f32),
            pltpu.VMEM((LANES + HEAD, width), bf16),
            pltpu.SemaphoreType.DMA((5,)),
        ],
        compiler_params=LIMIT,
        name="norm",
    )(*map(there, (inputs, norm_gain[None], out_hg_w, out_df_w)))
    rows = lax.all_to_all(normed, "fs", 0, 0, tiled=True)
    sources = (hg_query_w, hg_fwd_w, hg_bwd_w, hg_value_w, df_query_w, df_key_w, df_value_w)
    sent = pl.pallas_call(
        pack_kernel,
        in_specs=[FAR_SPEC] * 8,
        out_specs=vmem,
        out_shape=pltpu.VMEM((2, fs, packed + EXTRA, LANES), bf16),
        scratch_shapes=[
            pltpu.VMEM((4, depth, LANES), bf16),
            pltpu.VMEM((3, depth, LANES // 2), bf16),
            pltpu.VMEM((2, LANES), f32),
            pltpu.SemaphoreType.DMA((8,)),
        ],
        compiler_params=LIMIT,
        name="pack",
    )(*map(there, (*sources, floor_gap)))
    share = (lax.axis_index("tp") + z // 2) % 2
    both = lax.all_to_all(
        sent.reshape(2 * fs, packed + EXTRA, LANES),
        ("fs", "tp"),
        0,
        0,
        axis_index_groups=[
            [k * tp + 2 * x + c for c in range(2) for k in range(fs)] for x in range(tp // 2)
        ],
        tiled=True,
    )
    mine = lax.dynamic_slice_in_dim(both, share * fs, fs, 0)
    extra = mine[0, packed:]
    rings = [[k * tp + (t ^ (k // 2 % 2)) for k in range(sp)] for t in range(tp)]
    weights = lax.all_gather(
        mine[None, :, :packed], ("sp", "tp"), axis=0, tiled=True, axis_index_groups=rings
    )
    weights = weights.reshape(sp * fs, packed, LANES)
    projected = pl.pallas_call(
        project_kernel,
        in_specs=[SMEM_SPEC] + [vmem] * 2,
        out_specs=vmem,
        out_shape=pltpu.VMEM((2, fs, length + length // 2, LANES), bf16),
        scratch_shapes=[pltpu.VMEM((width, 2 * LANES), bf16)],
        compiler_params=LIMIT,
        name="project",
    )(y.astype(jnp.int32)[None], here(rows), here(weights))
    groups = [
        [((2 * i + a) * fs + k) * tp + t for a in range(2) for k in range(fs)]
        for i in range(sp // 2)
        for t in range(tp)
    ]
    got = lax.all_to_all(
        projected.reshape(2 * fs, length + length // 2, LANES),
        ("sp", "fs", "tp"),
        0,
        0,
        axis_index_groups=groups,
        tiled=True,
    )
    swap = [(k * tp + t, k * tp + (t ^ (k // 2 % 2))) for k in range(sp) for t in range(tp)]
    outer = lax.ppermute(outer, ("sp", "tp"), swap)

    place = z.astype(jnp.int32)[None]
    gains = jnp.concatenate([hg_norm_gain, hg_norm_gain, df_norm_gain, df_norm_gain])
    joined, other, query, local, read_fwd, read_bwd, gains = pl.pallas_call(
        local_kernel,
        in_specs=[SMEM_SPEC] * 2 + [vmem] * 3,
        out_specs=[vmem] * 7,
        out_shape=[
            pltpu.VMEM((length + HEAD + TAIL, LANES), bf16),
            pltpu.VMEM((2 * HEAD + TAIL, LANES), f32),
            pltpu.VMEM((length, LANES), bf16),
            pltpu.VMEM((length, LANES), f32),
            pltpu.VMEM((length, LANES), bf16),
            pltpu.VMEM((length, LANES), bf16),
            pltpu.VMEM((2, LANES), f32),
        ],
        compiler_params=LIMIT,
        name="local",
    )(place % 2, diff_lambda, here(got), here(extra), here(gains.reshape(2, LANES)))
    arrived = lax.all_gather(
        joined[None], ("sp", "tp"), axis=0, tiled=True, axis_index_groups=rings
    )
    partial = pl.pallas_call(
        finish_kernel,
        in_specs=[SMEM_SPEC] + [vmem] * 8,
        out_specs=vmem,
        out_shape=pltpu.VMEM((length, width), bf16),
        scratch_shapes=[pltpu.VMEM((length, LANES + HEAD), bf16)],
        compiler_params=LIMIT,
        name="finish",
    )(
        place,
        here(arrived),
        here(other),
        here(query),
        here(local),
        here(read_fwd),
        here(read_bwd),
        here(gains),
        here(outer),
    )
    parts = lax.all_to_all(
        partial.reshape(tp, length // tp, width), "tp", 0, 0, tiled=True
    )
    return pl.pallas_call(
        close_kernel,
        out_shape=jax.ShapeDtypeStruct((1, length // tp, width), bf16),
        compiler_params=LIMIT,
        name="close",
    )(here(parts), post_gain[None])


def solution(mesh):
    rows = P(("sp", "fs"), "tp")
    in_specs = (
        P("fs", "sp", None),
        P(),
        rows,
        rows,
        rows,
        rows,
        P(None, "tp"),
        P(),
        rows,
        rows,
        rows,
        P("tp"),
        P(),
        P("tp", None),
        P("tp", None),
        P(),
    )
    out_specs = P("fs", ("sp", "tp"), None)
    return jax.shard_map(shards, mesh=mesh, in_specs=in_specs, out_specs=out_specs, check_vma=False)
```

```python
import jax
import jax.numpy as jnp
from jax import lax
from jax.experimental import pallas as pl
from jax.experimental.pallas import tpu as pltpu
from jax.sharding import PartitionSpec as P

HEAD = 64
DQK = 32
LANES = 128
TAIL = 8
EXTRA = 16

epsilon = 1e-06
df_factor = 0.8
f32 = jnp.float32
bf16 = jnp.bfloat16

SMEM_SPEC = pl.BlockSpec(memory_space=pltpu.SMEM)
VMEM_SPEC = pl.BlockSpec(memory_space=pltpu.VMEM)
LIMIT = pltpu.CompilerParams(vmem_limit_bytes=24 * 2**20)


FAR_SPEC = pl.BlockSpec(memory_space=pltpu.HBM)


def there(array):
    return pltpu.with_memory_space_constraint(array, pltpu.HBM)


def here(array):
    return pltpu.with_memory_space_constraint(array, pltpu.VMEM)


def dot(a, b, dims, precision=None):
    return lax.dot_general(a, b, (dims, ((), ())), precision=precision, preferred_element_type=f32)


def thirds(value):
    pieces = []
    for _ in range(3):
        pieces.append(value.astype(bf16))
        value = value - pieces[-1].astype(f32)
    return pieces


def pack_kernel(q, f, b, v, dq, dk, dv, gaps_in, out, wide, narrow, gaps, sems):
    copies = [
        pltpu.make_async_copy(source, wide.at[j], sems.at[j])
        for j, source in enumerate((q, f, b, v))
    ] + [
        pltpu.make_async_copy(source, narrow.at[j], sems.at[4 + j])
        for j, source in enumerate((dq, dk, dv))
    ] + [pltpu.make_async_copy(gaps_in, gaps, sems.at[7])]
    for copy in copies:
        copy.start()
    for copy in copies:
        copy.wait()
    half = q.shape[0] // 2
    extra = stacked(EXTRA, (*thirds(gaps[0:1]), *thirds(gaps[1:2])))
    for j in range(4):
        k = j % 3
        folded = jnp.concatenate([narrow[k, :half, :], narrow[k, half:, :]], axis=1)
        block = jnp.concatenate([wide[j], folded, extra], axis=0)
        for c in range(2):
            out[c, j] = block


def norm_kernel(x, gain_in, hg_w, df_w, out, outer, rows, gain, joined, done, sems, out_sems):
    copies = (
        pltpu.make_async_copy(x.at[0], rows, sems.at[0]),
        pltpu.make_async_copy(gain_in, gain, sems.at[1]),
    )
    late = (
        pltpu.make_async_copy(hg_w, joined.at[:LANES], sems.at[2]),
        pltpu.make_async_copy(df_w, joined.at[LANES:], sems.at[3]),
    )
    for copy in (*copies, *late):
        copy.start()
    for copy in (*copies, *late):
        copy.wait()
    store = pltpu.make_async_copy(joined, outer, sems.at[4])
    store.start()
    chunks, step, _ = done.shape
    stores = [store]
    for c in range(chunks):
        part = rows[c * step : (c + 1) * step].astype(f32)
        scale = lax.rsqrt(jnp.mean(part * part, axis=-1, keepdims=True) + epsilon)
        done[c] = (part * scale * gain[...]).astype(bf16)
        for k in range(out.shape[0]):
            stores.append(
                pltpu.make_async_copy(
                    done.at[c], out.at[k, pl.ds(c * step, step)], out_sems.at[c, k]
                )
            )
            stores[-1].start()
    for store in stores:
        store.wait()


def project_kernel(place, rows, weights, out, rhs):
    blocks, packed, _ = weights.shape
    depth = packed * 2 // 3
    half = depth // 2
    wide = weights[:, :depth, :]
    narrow = weights[:, depth:, :].astype(f32)
    first, second = narrow[:, :, :HEAD], narrow[:, :, HEAD:]
    narrow = jnp.concatenate(
        [
            jnp.concatenate([first, first], axis=2),
            jnp.concatenate([second, second], axis=2),
        ],
        axis=1,
    ).astype(bf16)
    rhs[:, :LANES] = wide.reshape(blocks * depth, LANES)
    rhs[:, LANES:] = narrow.reshape(blocks * depth, LANES)
    count, length, width = rows.shape
    whole = dot(rows[...].reshape(count * length, width), rhs[...], ((1,), (0,))).astype(bf16)
    half = length // 2
    lane = lax.broadcasted_iota(jnp.int32, (half, LANES), 1)
    turned = jnp.where(place[0] == 2, HEAD, 0)
    early = lax.rem(lane + turned, LANES) < HEAD
    for k in range(count):
        part = whole[k * length : (k + 1) * length]
        folded = jnp.where(early, part[:half, LANES:], part[half:, LANES:])
        for a in range(2):
            out[a, k, :length] = part[:, :LANES]
            out[a, k, length:] = folded


def swapped(block):
    return jnp.concatenate([block[:, HEAD:], block[:, :HEAD]], axis=1)


def local_kernel(
    place, lam, got, extra_in, gains_in, out, other, query_out, local, read_fwd, read_bwd, gains
):
    extra = extra_in[...].astype(f32)
    gaps = [extra[3 * d : 3 * d + 1] + extra[3 * d + 1 : 3 * d + 2] + extra[3 * d + 2 : 3 * d + 3] for d in range(2)]
    gains[...] = gains_in[...]
    length = local.shape[0]
    half = length // 2
    odd = place[0] == 1
    mine = place[0] * 4
    row = lax.broadcasted_iota(jnp.int32, (length, length), 0)
    col = lax.broadcasted_iota(jnp.int32, (length, length), 1)
    lane = lax.broadcasted_iota(jnp.int32, (length, LANES), 1)
    lane_head = lax.broadcasted_iota(jnp.int32, (HEAD, LANES), 1)
    masks = row >= col, row <= col
    takens, gones, states, decays = ({}, {}, {}, {})
    for slot in range(2):
        values = got[4 * slot + 3, :length]
        for d in range(2):
            gate = got[4 * slot + 1 + d, :length].astype(f32)
            taken = gaps[d] * jax.nn.sigmoid(-gate)
            kept = jnp.log1p(-taken)
            gone = dot(masks[d].astype(f32), kept, ((1,), (0,)), lax.Precision.HIGHEST)
            total = gone[length - 1 : length] if d == 0 else gone[0:1]
            state = dot(values, (taken * jnp.exp(total - gone)).astype(bf16), ((0,), (0,)))
            takens[slot, d], gones[slot, d] = taken, gone
            states[slot, d] = jnp.where(lane_head < HEAD, state[:HEAD], state[HEAD:])
            decays[slot, d] = jnp.exp(total)
    fwd = decays[1, 0] * states[0, 0] + states[1, 0]
    bwd = decays[0, 1] * states[1, 1] + states[0, 1]
    quarter = HEAD // 2
    part = jnp.concatenate(
        [
            jnp.where(odd, fwd[quarter:], fwd[:quarter]),
            jnp.where(odd, bwd[quarter:], bwd[:quarter]),
        ],
        axis=0,
    )
    out[length : length + HEAD] = part.astype(bf16)
    lines = (*halves(decays[0, 0] * decays[1, 0]), *halves(decays[0, 1] * decays[1, 1]))
    lines = (*lines, *thirds(jnp.full((1, LANES), lam[0], f32)))
    out[length + HEAD :] = stacked(TAIL, lines)
    other[:HEAD] = states[0, 0]
    other[HEAD : 2 * HEAD] = states[1, 1]
    row_tail = lax.broadcasted_iota(jnp.int32, (TAIL, LANES), 0)
    other[2 * HEAD :] = jnp.where(row_tail == 0, decays[0, 0], decays[1, 1])

    keys, worth = got[mine + 1, length:], got[mine + 2, length:]
    lane_half = lane[:half]
    out[:half] = jnp.where(lane_half < HEAD, keys, worth)
    out[half:length] = swapped(jnp.where(lane_half < HEAD, worth, keys))
    folded = got[mine, length:]
    query_out[:half] = folded
    query_out[half:] = swapped(folded)

    queries = got[mine, :length].astype(f32)
    queries = queries * jax.nn.sigmoid(queries)
    values = got[mine + 3, :length]
    weights = [0.0, 0.0]
    for d in range(2):
        gone = jnp.where(odd, gones[1, d], gones[0, d])
        taken = jnp.where(odd, takens[1, d], takens[0, d])
        reader = read_bwd if d else read_fwd
        reader[...] = (queries * jnp.exp(gone)).astype(bf16)
        middle = gone[half : half + 1]
        query_part = queries * jnp.exp(gone - middle)
        key_part = (taken * jnp.exp(middle - gone)).astype(bf16)
        for h in range(2):
            inside = (lane >= h * HEAD) & (lane < (h + 1) * HEAD)
            score = dot(jnp.where(inside, query_part, 0.0).astype(bf16), key_part, ((1,), (1,)))
            weights[h] = weights[h] + jnp.where(masks[d], score, 0.0)
    out_0 = dot(weights[0].astype(bf16), values, ((1,), (0,)))
    out_1 = dot(weights[1].astype(bf16), values, ((1,), (0,)))
    local[...] = jnp.where(lane < HEAD, out_0, out_1)


def stacked(count, lines):
    row = lax.broadcasted_iota(jnp.int32, (count, LANES), 0)
    block = jnp.zeros((count, LANES), f32)
    for k, line in enumerate(lines):
        block = jnp.where(row == k, jnp.broadcast_to(line.astype(f32), (count, LANES)), block)
    return block.astype(bf16)


def halves(value):
    high = value.astype(bf16)
    return high, (value - high.astype(f32)).astype(bf16)


def finish_kernel(
    place, got, other, df_query, local, read_fwd, read_bwd, gains, outer, out, mixed
):
    devices = got.shape[0]
    length = local.shape[0]
    me = place[0]
    lane = lax.broadcasted_iota(jnp.int32, (length, LANES), 1)

    half = HEAD // 2
    pair, odd = me // 2, lax.rem(me, 2) == 1

    def folded(order, passed, k):
        state = jnp.zeros((HEAD, LANES), f32)
        rows = slice(length + k * half, length + (k + 1) * half)
        for w in order:
            fresh = jnp.concatenate([got[2 * w, rows], got[2 * w + 1, rows]], axis=0).astype(f32)
            tail = got[2 * w, length + HEAD :].astype(f32)
            decay = tail[2 * k : 2 * k + 1] + tail[2 * k + 1 : 2 * k + 2]
            state = jnp.where(passed(w), decay * state + fresh, state)
        decay = other[2 * HEAD + k : 2 * HEAD + k + 1]
        joined = decay * state + other[k * HEAD : (k + 1) * HEAD]
        return jnp.where(odd if k == 0 else jnp.logical_not(odd), joined, state).astype(bf16)

    fwd = folded(range(devices // 2), lambda w: w < pair, 0)
    bwd = folded(range(devices // 2 - 1, -1, -1), lambda w: w > pair, 1)
    recurrent = local[...]
    parts = []
    for h in range(2):
        inside = (lane >= h * HEAD) & (lane < (h + 1) * HEAD)
        zero = jnp.zeros((length, LANES), bf16)
        parts.append(
            dot(jnp.where(inside, read_fwd[...], zero), fwd, ((1,), (1,)))
            + dot(jnp.where(inside, read_bwd[...], zero), bwd, ((1,), (1,)))
        )
    recurrent = recurrent + jnp.concatenate(parts, axis=1)
    squares = recurrent * recurrent
    first = jnp.sum(jnp.where(lane < HEAD, squares, 0.0), axis=1, keepdims=True)
    second = jnp.sum(jnp.where(lane < HEAD, 0.0, squares), axis=1, keepdims=True)
    mean = jnp.where(lane < HEAD, first, second) * (1.0 / HEAD)
    mixed[:, :LANES] = (recurrent * lax.rsqrt(mean + epsilon) * gains[0:1]).astype(bf16)

    keys_values = got[:, :length, :].reshape(devices * length, LANES)
    query = df_query[...]
    only = jnp.concatenate(
        [
            jnp.where((lane >= m * DQK) & (lane < (m + 1) * DQK), query, jnp.zeros_like(query))
            for m in range(2)
        ],
        axis=0,
    )
    scores = dot(only, keys_values, ((1,), (1,))) * (DQK ** (-0.5))
    shifted = jnp.exp(scores - jnp.max(scores, axis=-1, keepdims=True))
    totals = jnp.sum(shifted, axis=-1, keepdims=True)
    maps = dot(shifted.astype(bf16), keys_values, ((1,), (0,))) / totals
    first = got[0, length + HEAD :].astype(f32)
    lam = first[4:5] + first[5:6] + first[6:7]
    weighted = (maps[:length] - lam * maps[length:])[:, HEAD:]
    mean = jnp.mean(weighted * weighted, axis=-1, keepdims=True)
    mixed[:, LANES:] = (
        weighted * lax.rsqrt(mean + epsilon) * gains[1:2, :HEAD] * df_factor
    ).astype(bf16)
    out[...] = dot(mixed[...], outer[...], ((1,), (0,))).astype(bf16)


def close_kernel(parts, gain, out):
    mixture = parts[0].astype(f32)
    for k in range(1, parts.shape[0]):
        mixture = mixture + parts[k].astype(f32)
    scale = lax.rsqrt(jnp.mean(mixture * mixture, axis=-1, keepdims=True) + epsilon)
    out[0] = (mixture * scale * gain[...]).astype(bf16)


def shards(
    inputs,
    norm_gain,
    hg_query_w,
    hg_fwd_w,
    hg_bwd_w,
    hg_value_w,
    floor_gap,
    hg_norm_gain,
    df_query_w,
    df_key_w,
    df_value_w,
    diff_lambda,
    df_norm_gain,
    out_hg_w,
    out_df_w,
    post_gain,
):
    sp, fs, tp = (lax.axis_size(a) for a in ("sp", "fs", "tp"))
    z, y = lax.axis_index("sp"), lax.axis_index("fs")
    _, length, width = inputs.shape
    depth = hg_query_w.shape[0]
    packed = depth + depth // 2

    vmem = VMEM_SPEC
    normed, outer = pl.pallas_call(
        norm_kernel,
        in_specs=[FAR_SPEC] * 4,
        out_specs=[FAR_SPEC] * 2,
        out_shape=[
            pltpu.HBM((fs, length, width), bf16),
            pltpu.HBM((LANES + HEAD, width), bf16),
        ],
        scratch_shapes=[
            pltpu.VMEM((length, width), bf16),
            pltpu.VMEM((1, width), f32),
            pltpu.VMEM((LANES + HEAD, width), bf16),
            pltpu.VMEM((4, length // 4, width), bf16),
            pltpu.SemaphoreType.DMA((5,)),
            pltpu.SemaphoreType.DMA((4, fs)),
        ],
        compiler_params=LIMIT,
        name="norm",
    )(*map(there, (inputs, norm_gain[None], out_hg_w, out_df_w)))
    rows = lax.all_to_all(normed, "fs", 0, 0, tiled=True)
    sources = (hg_query_w, hg_fwd_w, hg_bwd_w, hg_value_w, df_query_w, df_key_w, df_value_w)
    sent = pl.pallas_call(
        pack_kernel,
        in_specs=[FAR_SPEC] * 8,
        out_specs=vmem,
        out_shape=pltpu.VMEM((2, fs, packed + EXTRA, LANES), bf16),
        scratch_shapes=[
            pltpu.VMEM((4, depth, LANES), bf16),
            pltpu.VMEM((3, depth, LANES // 2), bf16),
            pltpu.VMEM((2, LANES), f32),
            pltpu.SemaphoreType.DMA((8,)),
        ],
        compiler_params=LIMIT,
        name="pack",
    )(*map(there, (*sources, floor_gap)))
    share = (lax.axis_index("tp") + z // 2) % 2
    both = lax.all_to_all(
        sent.reshape(2 * fs, packed + EXTRA, LANES),
        ("fs", "tp"),
        0,
        0,
        axis_index_groups=[
            [k * tp + 2 * x + c for c in range(2) for k in range(fs)] for x in range(tp // 2)
        ],
        tiled=True,
    )
    mine = lax.dynamic_slice_in_dim(both, share * fs, fs, 0)
    extra = mine[0, packed:]
    rings = [[k * tp + (t ^ (k // 2 % 2)) for k in range(sp)] for t in range(tp)]
    weights = lax.all_gather(
        mine[None, :, :packed], ("sp", "tp"), axis=0, tiled=True, axis_index_groups=rings
    )
    weights = weights.reshape(sp * fs, packed, LANES)
    projected = pl.pallas_call(
        project_kernel,
        in_specs=[SMEM_SPEC] + [vmem] * 2,
        out_specs=vmem,
        out_shape=pltpu.VMEM((2, fs, length + length // 2, LANES), bf16),
        scratch_shapes=[pltpu.VMEM((width, 2 * LANES), bf16)],
        compiler_params=LIMIT,
        name="project",
    )(y.astype(jnp.int32)[None], here(rows), here(weights))
    groups = [
        [((2 * i + a) * fs + k) * tp + t for a in range(2) for k in range(fs)]
        for i in range(sp // 2)
        for t in range(tp)
    ]
    got = lax.all_to_all(
        projected.reshape(2 * fs, length + length // 2, LANES),
        ("sp", "fs", "tp"),
        0,
        0,
        axis_index_groups=groups,
        tiled=True,
    )
    swap = [(k * tp + t, k * tp + (t ^ (k // 2 % 2))) for k in range(sp) for t in range(tp)]
    outer = lax.ppermute(outer, ("sp", "tp"), swap)

    place = z.astype(jnp.int32)[None]
    gains = jnp.concatenate([hg_norm_gain, hg_norm_gain, df_norm_gain, df_norm_gain])
    joined, other, query, local, read_fwd, read_bwd, gains = pl.pallas_call(
        local_kernel,
        in_specs=[SMEM_SPEC] * 2 + [vmem] * 3,
        out_specs=[vmem] * 7,
        out_shape=[
            pltpu.VMEM((length + HEAD + TAIL, LANES), bf16),
            pltpu.VMEM((2 * HEAD + TAIL, LANES), f32),
            pltpu.VMEM((length, LANES), bf16),
            pltpu.VMEM((length, LANES), f32),
            pltpu.VMEM((length, LANES), bf16),
            pltpu.VMEM((length, LANES), bf16),
            pltpu.VMEM((2, LANES), f32),
        ],
        compiler_params=LIMIT,
        name="local",
    )(place % 2, diff_lambda, here(got), here(extra), here(gains.reshape(2, LANES)))
    arrived = lax.all_gather(
        joined[None], ("sp", "tp"), axis=0, tiled=True, axis_index_groups=rings
    )
    partial = pl.pallas_call(
        finish_kernel,
        in_specs=[SMEM_SPEC] + [vmem] * 8,
        out_specs=vmem,
        out_shape=pltpu.VMEM((length, width), bf16),
        scratch_shapes=[pltpu.VMEM((length, LANES + HEAD), bf16)],
        compiler_params=LIMIT,
        name="finish",
    )(
        place,
        here(arrived),
        here(other),
        here(query),
        here(local),
        here(read_fwd),
        here(read_bwd),
        here(gains),
        here(outer),
    )
    parts = lax.all_to_all(
        partial.reshape(tp, length // tp, width), "tp", 0, 0, tiled=True
    )
    return pl.pallas_call(
        close_kernel,
        out_shape=jax.ShapeDtypeStruct((1, length // tp, width), bf16),
        compiler_params=LIMIT,
        name="close",
    )(here(parts), post_gain[None])


def solution(mesh):
    rows = P(("sp", "fs"), "tp")
    in_specs = (
        P("fs", "sp", None),
        P(),
        rows,
        rows,
        rows,
        rows,
        P(None, "tp"),
        P(),
        rows,
        rows,
        rows,
        P("tp"),
        P(),
        P("tp", None),
        P("tp", None),
        P(),
    )
    out_specs = P("fs", ("sp", "tp"), None)
    return jax.shard_map(shards, mesh=mesh, in_specs=in_specs, out_specs=out_specs, check_vma=False)
```
